256 devices in a mesh: sp: 64 (over z, x, core), tp: 4 (over y).
Axes of the slice: x: 4, y: 4, z: 8, core: 2. Of those that a mesh axis runs over, the one named last changes fastest.
Arguments:
- query_one: bfloat16 [16384, 512], P('sp', 'tp'), may hold values from -100 to 100, as said below
- key_one: bfloat16 [16384, 512], P('sp', 'tp'), may hold values from -8 to 8
- query_two: bfloat16 [16384, 512], P('sp', 'tp'), may hold values from -100 to 100, as said below
- key_two: bfloat16 [16384, 512], P('sp', 'tp'), may hold values from -8 to 8
- values: bfloat16 [16384, 1024], P('sp', 'tp'), may hold values from -6 to 6
- mix_lambda: float32 [8], P('tp'), may hold values from 0.3 to 0.8
- head_gain: float32 [128], replicated, may hold values from 0.1 to 1.9
- residual_in: bfloat16 [16384, 2048], P(('sp', 'tp')), may hold values from -6 to 6
- out_weight: bfloat16 [1024, 2048], replicated, may hold values from -0.1875 to 0.1875
- norm_gain: float32 [2048], replicated, may hold values from 0.1 to 1.9
- route_ids: int32 [16384, 2], P(('sp', 'tp')), may hold values from 0 to 127, all different within a row; in each aligned block of 64 rows (0 to 63, 64 to 127, ...) at most 2 rows name the same one
- route_logits: float32 [16384, 2], P(('sp', 'tp')), may hold values from -6 to 6
- group_prob: float32 [16384], P(('sp', 'tp')), may hold values from 0.25 to 1
- gate_weight: bfloat16 [128, 2048, 1024], P('sp', None, 'tp'), may hold values from -0.125 to 0.125
- up_weight: bfloat16 [128, 2048, 1024], P('sp', None, 'tp'), may hold values from -0.125 to 0.125
- down_weight: bfloat16 [128, 1024, 2048], P('sp', 'tp'), may hold values from -0.1875 to 0.1875
Outputs:
- layer_out: bfloat16 [16384, 2048], P(('sp', 'tp'))
The draws below stay inside these ranges and needn't reach their ends.
Inputs may be any that keep to these rules, and one draw needn't show every extreme that they name: `query_one`: drawn together with key_one. `query_two`: drawn together with key_two. `route_ids`: the experts of a row differ. In the rows of one device no expert is named more than 2 times, a bound that some block reaches.
All inputs are finite; a program needn't handle non-finite values.
Results may differ from the reference program's by a relative error of at most 0.014.
Values may be sent and summed in bfloat16 or wider, within the bound.
A program may use at most 128 MiB of HBM per device.

```python
import math
import jax
import jax.numpy as jnp
import numpy as np
from jax import lax

D = 2048
HEADS = 8
QK = 64
VD = 128
FF = 1024
TOP = 2
ROWS = 64
TOKENS = 16384
MIXW = 1024
EXPERTS = 128
CAP = 2
N_SP = 64
N_TP = 4


def draw_maps(key, which):
    streams = jax.random.split(jax.random.fold_in(key, which), 2)
    keys_drawn = 1.3 * jax.random.normal(streams[0], (TOKENS, HEADS * QK), jnp.float32)
    queries = 1.3 * jax.random.normal(streams[1], (TOKENS, HEADS * QK), jnp.float32)
    queries = jnp.clip(queries, -100.0, 100.0)
    keys_drawn = jnp.clip(keys_drawn, -8.0, 8.0)
    return (queries, keys_drawn)


def draw_query_one(key, part):
    return draw_maps(key, 11)[0].astype(jnp.bfloat16)


def draw_key_one(key, part):
    return draw_maps(key, 11)[1].astype(jnp.bfloat16)


def draw_query_two(key, part):
    return draw_maps(key, 23)[0].astype(jnp.bfloat16)


def draw_key_two(key, part):
    return draw_maps(key, 23)[1].astype(jnp.bfloat16)


def levels(key, shape, cuts, low, top_value):
    loudness = 1.0
    for position, parts in cuts:
        steps = jax.random.uniform(jax.random.fold_in(jax.random.fold_in(key, 6), position), (parts,), jnp.float32, low / len(cuts), top_value / len(cuts))
        loudness = loudness * jnp.repeat(jnp.exp(steps), shape[position] // parts).reshape((-1,) + (1,) * (len(shape) - 1 - position))
    return loudness


def deal_out(stream_key, own, number, rows, count, top, most, slope):
    sequence = jax.random.permutation(stream_key, count)
    crowded, common = load_shares(count, rows * top, most, slope, True), load_shares(count, rows * top, most, slope, False)
    places = jnp.arange(count)

    def named(sizes, rotation):
        used = int((sizes > 0).sum())
        fixed = max(1, used // 4)
        passed = fixed + (places - fixed + rotation * (used - fixed)) % max(1, count - fixed)
        return jnp.zeros((count,), jnp.int32).at[sequence[jnp.where(places < fixed, places, passed)]].set(jnp.asarray(sizes, jnp.int32))

    sizes = jnp.where(number % 4 == 0, named(crowded, number // 4), named(common, number - number // 4 - 1))
    mixed = jax.random.permutation(jax.random.fold_in(own, 3), count)
    donor, taker = mixed[0:count // 2 * 2:2], mixed[1:count // 2 * 2:2]
    slack = jnp.minimum(sizes[donor] - 1, most - sizes[taker]) // 2
    slack = jnp.where((donor == sequence[0]) | (taker == sequence[0]) | (sizes[taker] == 0), 0, jnp.maximum(slack, 0))
    passed = jax.random.randint(jax.random.fold_in(own, 4), (count // 2,), 0, 1 << 20) % (slack + 1)
    sizes = sizes.at[donor].add(-passed).at[taker].add(passed)
    labels = jnp.searchsorted(jnp.cumsum(sizes), jnp.arange(rows * top), side="right").astype(jnp.int32)
    grid = labels.reshape(top, rows).T
    grid = grid[jax.random.permutation(jax.random.fold_in(own, 1), rows)]
    rotation = jax.random.randint(jax.random.fold_in(own, 2), (rows, 1), 0, top)
    return jnp.take_along_axis(grid, (jnp.arange(top)[None, :] + rotation) % top, axis=1)


def load_shares(count, total, most, lean, full):
    portions = [(1 << 20) // math.isqrt(rank ** lean) + 1 for rank in range(1, count + 1)]
    largest = most if full else min(most, max(-(-total // count), total * portions[0] // sum(portions)))
    least = 1 if total - largest >= count - 1 else 0
    given, surplus = [largest] + [least] * (count - 1), total - largest - least * (count - 1)
    while surplus > 0:
        movable = [i for i in range(1, count) if given[i] < largest] or [i for i in range(1, count) if given[i] < most]
        pool, budget = sum([portions[i] for i in movable]), surplus
        for i in movable:
            more = min(most - given[i], max(1, budget * portions[i] // pool), surplus)
            given[i] = given[i] + more
            surplus = surplus - more
    return np.array(given)


def normal_values(key, shape, spread, reach, shards=(), held_as=jnp.bfloat16):
    entries = jax.random.normal(key, shape, jnp.float32) * spread
    if len(shards) > 0:
        entries = levels(key, shape, shards, -0.22, 0.18) * entries
    return jnp.clip(entries, min=-reach, max=reach).astype(held_as)


def setup_inputs(seed: int = 0) -> dict:
    splits = jax.random.split(jax.random.key(seed), 17)
    query_one = draw_query_one(jax.random.fold_in(splits[16], 71), 0)
    key_one = draw_key_one(jax.random.fold_in(splits[16], 71), 0)
    query_two = draw_query_two(jax.random.fold_in(splits[16], 71), 0)
    key_two = draw_key_two(jax.random.fold_in(splits[16], 71), 0)
    values = normal_values(splits[4], (TOKENS, MIXW), 1.0, 6.0, ((0, 64), (1, 4)))
    mix_lambda = jnp.clip(0.3 + 0.5 * jax.random.uniform(splits[5], (HEADS,), jnp.float32) ** levels(splits[5], (HEADS,), ((0, 4),), -0.2, 0.2), 0.3, 0.8)
    head_gain = jnp.clip(1.0 + 0.18 * jax.random.normal(splits[6], (VD,), jnp.float32), 0.1, 1.9)
    residual_in = normal_values(splits[7], (TOKENS, D), 1.0, 6.0, ((0, 256),))
    out_weight = normal_values(splits[8], (MIXW, D), MIXW ** -0.5, 0.1875)
    norm_gain = jnp.clip(1.0 + 0.18 * jax.random.normal(splits[9], (D,), jnp.float32), 0.1, 1.9)
    route_ids_keys = jax.random.split(jax.random.fold_in(splits[10], 1), TOKENS // ROWS)
    route_ids_turns = jax.random.permutation(jax.random.fold_in(splits[10], 3), TOKENS // ROWS)
    route_ids = jax.vmap(lambda own, number: deal_out(jax.random.fold_in(splits[10], 2), own, number, ROWS, EXPERTS, TOP, CAP, 2))(route_ids_keys, route_ids_turns).reshape((TOKENS, TOP))
    route_logits = normal_values(splits[11], (TOKENS, TOP), 1.0, 6.0, ((0, 256),), jnp.float32)
    group_prob = jnp.clip(0.25 + 0.75 * jax.random.uniform(splits[12], (TOKENS,), jnp.float32) ** levels(splits[12], (TOKENS,), ((0, 256),), -0.2, 0.2), 0.25, 1.0)
    gate_weight = normal_values(splits[13], (EXPERTS, D, FF), D ** -0.5, 0.125, ((0, 64), (2, 4)))
    up_weight = normal_values(splits[14], (EXPERTS, D, FF), D ** -0.5, 0.125, ((0, 64), (2, 4)))
    down_weight = normal_values(splits[15], (EXPERTS, FF, D), FF ** -0.5, 0.1875, ((0, 64), (1, 4)))
    return {"query_one": query_one, "key_one": key_one, "query_two": query_two, "key_two": key_two, "values": values, "mix_lambda": mix_lambda, "head_gain": head_gain, "residual_in": residual_in, "out_weight": out_weight, "norm_gain": norm_gain, "route_ids": route_ids, "route_logits": route_logits, "group_prob": group_prob, "gate_weight": gate_weight, "up_weight": up_weight, "down_weight": down_weight}


norm_epsilon = 1e-06

def round_kept(value):
    return lax.optimization_barrier(value.astype(jnp.bfloat16)).astype(jnp.float32)

def head_output(query_a, key_a, query_b, key_b, head_values, weight_two, gain):
    score_scale = 1.0 / math.sqrt(QK)
    block_rows = min(512, TOKENS)

    def one_map(queries, keys):
        scores = jnp.dot(queries, keys.T, preferred_element_type=jnp.float32) * score_scale
        top_score = lax.optimization_barrier(jnp.max(scores, axis=-1, keepdims=True))
        expo = jnp.exp(scores - top_score)
        summed = lax.optimization_barrier(jnp.sum(expo, axis=-1, keepdims=True))
        return jnp.dot(expo.astype(jnp.bfloat16), head_values, preferred_element_type=jnp.float32) / summed

    def one_block(pair):
        block_a, block_b = pair
        combined = one_map(block_a, key_a) - weight_two * one_map(block_b, key_b)
        combined = combined * lax.rsqrt(lax.optimization_barrier(jnp.mean(combined * combined, axis=-1, keepdims=True)) + norm_epsilon) * gain
        return combined.astype(jnp.bfloat16)
    blocks = lax.map(one_block, (query_a.reshape(TOKENS // block_rows, block_rows, QK), query_b.reshape(TOKENS // block_rows, block_rows, QK)))
    return blocks.reshape(TOKENS, VD)

def reference(query_one, key_one, query_two, key_two, values, mix_lambda, head_gain, residual_in, out_weight, norm_gain, route_ids, route_logits, group_prob, gate_weight, up_weight, down_weight):

    def by_head(array, size):
        return array.reshape(TOKENS, HEADS, size).transpose(1, 0, 2)

    def run_head(packed):
        qa, ka, qb, kb, vals, weight_two = packed
        return head_output(qa, ka, qb, kb, vals, weight_two, head_gain)
    heads_out = lax.map(run_head, (by_head(query_one, QK), by_head(key_one, QK), by_head(query_two, QK), by_head(key_two, QK), by_head(values, VD), mix_lambda))
    attended = heads_out.transpose(1, 0, 2).reshape(TOKENS, MIXW)
    mix = jnp.dot(attended, out_weight, preferred_element_type=jnp.float32)
    hidden = (residual_in.astype(jnp.float32) + mix).astype(jnp.bfloat16)
    hidden_f = hidden.astype(jnp.float32)
    normed = (hidden_f * lax.rsqrt(lax.optimization_barrier(jnp.mean(hidden_f * hidden_f, axis=-1, keepdims=True)) + norm_epsilon) * norm_gain).astype(jnp.bfloat16)
    route_weight = jax.nn.softmax(route_logits, axis=-1) * group_prob[:, None]
    flat_ids = route_ids.reshape(-1)
    flat_weight = route_weight.reshape(-1)
    limit = CAP * N_SP * N_TP
    positions = jnp.arange(TOKENS * TOP, dtype=jnp.int32)
    block_ff = FF // N_TP

    def expert_step(running, expert):
        hit = flat_ids == expert
        rank = jnp.cumsum(hit.astype(jnp.int32)) - 1
        where_to = jnp.where(hit, rank, limit).astype(jnp.int32)
        chosen = jnp.zeros((limit,), jnp.int32).at[where_to].set(positions, mode='drop')
        live = jnp.zeros((limit,), jnp.float32).at[where_to].set(1.0, mode='drop')
        token_of = chosen // TOP
        picked = normed[token_of]
        gate = jnp.dot(picked, gate_weight[expert], preferred_element_type=jnp.float32)
        upper = jnp.dot(picked, up_weight[expert], preferred_element_type=jnp.float32)
        middle = (jax.nn.silu(gate) * upper).astype(jnp.bfloat16)
        down = down_weight[expert]
        summed = jnp.zeros((limit, D), jnp.float32)
        for piece in range(N_TP):
            part_sum = jnp.dot(middle[:, piece * block_ff:(piece + 1) * block_ff], down[piece * block_ff:(piece + 1) * block_ff], preferred_element_type=jnp.float32)
            summed = summed + round_kept(part_sum)
        expert_out = round_kept(summed)
        scaled = expert_out * (flat_weight[chosen] * live)[:, None]
        return (running.at[token_of].add(scaled), None)
    moe, _ = lax.scan(expert_step, jnp.zeros((TOKENS, D), jnp.float32), jnp.arange(EXPERTS, dtype=jnp.int32))
    return (hidden_f + moe).astype(jnp.bfloat16)
```

```python
import functools
import math

import jax
import jax.numpy as jnp
from jax import lax
from jax.experimental import pallas as pl
from jax.experimental.pallas import tpu as pltpu
from jax.sharding import PartitionSpec as P

norm_epsilon = 1e-06
MESH = pl.DeviceIdType.MESH
log2_e = math.log2(math.e)

NZ, NX = 8, 4
ROWS_A, ROWS_B = 96, 160
HALF_A, HALF_B = ROWS_A // 2, ROWS_B // 2
UNIT_ORDER = (0, 1, 7, 2, 6, 3, 5, 4)


def gather_plan():
    rate, lag = 46.6, 2.0
    ready, links, sends = {}, {}, []

    def rows_of(piece):
        kind, _, _, part = piece
        whole, half = (ROWS_A, HALF_A) if kind == "A" else (ROWS_B, HALF_B)
        return whole if part < 0 else half

    def follow(piece):
        kind, dz, slot, part = piece
        out = []
        if kind == "A":
            if dz == 0:
                if slot == 0:
                    out += [("x+", ("A", 0, 2, -1), -1), ("x-", ("A", 0, 1, -1), -1)]
                if slot == 2:
                    out.append(("x+", ("A", 0, 3, 0), 0))
                if slot == 1:
                    out.append(("x-", ("A", 0, 3, 1), 1))
                out += [("z+", ("A", 7, slot, part), part), ("z-", ("A", 1, slot, part), part)]
            elif dz in (7, 6) or (dz == 5 and slot < 2):
                out.append(("z+", ("A", dz - 1, slot, part), part))
            elif dz in (1, 2) or (dz == 3 and slot >= 2):
                out.append(("z-", ("A", dz + 1, slot, part), part))
            return out
        if slot == 0:
            if dz == 0:
                out += [("z+", ("B", 7, 0, -1), -1), ("z-", ("B", 1, 0, -1), -1)]
            elif dz in (7, 6):
                out.append(("z+", ("B", dz - 1, 0, -1), -1))
            elif dz in (1, 2):
                out.append(("z-", ("B", dz + 1, 0, -1), -1))
            elif dz == 5:
                out.append(("z+", ("B", 4, 0, 0), 0))
            elif dz == 3:
                out.append(("z-", ("B", 4, 0, 1), 1))
            out += [("x+", ("B", dz, 2, part), part), ("x-", ("B", dz, 1, part), part)]
        elif slot == 2 and dz < 4:
            out.append(("x+", ("B", dz, 3, part), part))
        elif slot == 1 and dz >= 4:
            out.append(("x-", ("B", dz, 3, part), part))
        return out

    events = [(0.0, 1, ("B", 0, 0, -1)), (0.0, 0, ("A", 0, 0, -1))]
    order = []
    while events:
        events.sort()
        now, _, piece = events.pop(0)
        order.append((now, piece, follow(piece)))
        for link, target, _ in follow(piece):
            begin = max(links.get(link, 0.0), now)
            links[link] = begin + rows_of(target) / rate
            events.append((links[link] + lag, len(order), target))
    return order


PLAN = gather_plan()
PIECES = [piece for _, piece, _ in PLAN]
PIECE_INDEX = {piece: n for n, piece in enumerate(PIECES)}
COMPUTE_US = 2.3


def unit_slots():
    units = [(kind, dz) for dz in UNIT_ORDER for kind in ("B", "A")]
    slots, clock, taken = [], 0.0, 0
    for kind, dz in units:
        need = max(t for t, piece, _ in PLAN if piece[0] == kind and piece[1] == dz) + 1.0
        clock = max(clock, need)
        mine = []
        while taken < len(PLAN) and PLAN[taken][0] <= clock:
            mine.append(taken)
            taken += 1
        slots.append(mine)
        clock += COMPUTE_US * (ROWS_A if kind == "A" else ROWS_B) / 128
    assert taken == len(PLAN)
    return units, slots


UNITS, SLOTS = unit_slots()


def attend_kernel(
    q1_ref, q2_ref, k1_ref, k2_ref, v_ref, lam_ref, gain_ref, gate_ref, up_ref, down_ref,
    out_ref, wg_ref, wu_ref, wd_ref, rg_ref, ru_ref, rd_ref,
    kva, kvb, qt, m_ref, l_ref, acc_ref, att,
    load_sem, send_sem, recv_sem, pass_sem, got_sem, head_send, head_recv,
    ws_sem, wr_sem, wl_sem, relay_sem, relay_send, pair_send, pair_recv,
):
    sp = lax.axis_index("sp")
    y = lax.axis_index("tp")
    core = lax.rem(sp, 2)
    x = lax.rem(sp // 2, NX)
    z = sp // (2 * NX)

    def place(zz, xx, cc):
        return (zz * NX + xx) * 2 + cc

    peers = {
        "x+": (place(z, lax.rem(x + 1, NX), core), y),
        "x-": (place(z, lax.rem(x + NX - 1, NX), core), y),
        "z+": (place(lax.rem(z + 1, NZ), x, core), y),
        "z-": (place(lax.rem(z + NZ - 1, NZ), x, core), y),
        "pair": (place(z, x, 1 - core), y),
        "y1": (sp, lax.rem(y + 1, 4)),
        "y2": (sp, lax.rem(y + 2, 4)),
        "y3": (sp, lax.rem(y + 3, 4)),
    }

    loads = []
    for n, (buf, low, high) in enumerate(((kvb, ROWS_A, 256), (kva, 0, ROWS_A))):
        for c, (ref, lo, hi) in enumerate(((k1_ref, 0, 128), (k2_ref, 128, 256), (v_ref, 256, 512))):
            copy = pltpu.make_async_copy(
                ref.at[low:high], buf.at[0, 0, 0, :, lo:hi], load_sem.at[n * 3 + c]
            )
            copy.start()
            loads.append(copy)

    barrier = pltpu.get_barrier_semaphore()
    for peer in peers.values():
        pl.semaphore_signal(barrier, inc=1, device_id=peer, device_id_type=MESH)
    pl.semaphore_wait(barrier, len(peers))

    def region(piece, side):
        kind, dz, slot, part = piece
        buf, half = (kva, HALF_A) if kind == "A" else (kvb, HALF_B)
        ref = buf.at[dz, side, slot]
        return ref if part < 0 else ref.at[part * half:(part + 1) * half]

    def part_of(piece, part):
        kind, dz, slot, own = piece
        return region(piece, 0) if part == own else region((kind, dz, slot, part), 0)

    def copy_on(piece, link, target, part):
        n = PIECE_INDEX[target]
        return pltpu.make_async_remote_copy(
            src_ref=part_of(piece, part), dst_ref=region(target, 0),
            send_sem=send_sem.at[n], recv_sem=recv_sem.at[n],
            device_id=peers[link], device_id_type=MESH,
        )

    def hand_over(piece):
        n = PIECE_INDEX[piece]
        return pltpu.make_async_remote_copy(
            src_ref=region(piece, 0), dst_ref=region(piece, 1),
            send_sem=pass_sem.at[n], recv_sem=got_sem.at[n],
            device_id=peers["pair"], device_id_type=MESH,
        )

    def arrive(piece):
        n = PIECE_INDEX[piece]
        pltpu.make_async_remote_copy(
            src_ref=region(piece, 0), dst_ref=region(piece, 0),
            send_sem=send_sem.at[n], recv_sem=recv_sem.at[n],
            device_id=peers["pair"], device_id_type=MESH,
        ).wait_recv()

    weights = ((gate_ref, wg_ref, rg_ref), (up_ref, wu_ref, ru_ref), (down_ref, wd_ref, rd_ref))
    home = y // 2 == core
    relay_plus = lax.rem(y + 1, 4) // 2 == core

    def half_of(ref, half):
        rows = ref.shape[0] // 2
        return ref.at[half * rows:(half + 1) * rows]

    def far_copy(a, j, half):
        src, _, relay = weights[a]
        return pltpu.make_async_remote_copy(
            src_ref=half_of(src.at[j], half), dst_ref=relay,
            send_sem=ws_sem.at[2 + half, a], recv_sem=relay_sem.at[a],
            device_id=peers["y1" if half == 0 else "y3"], device_id_type=MESH,
        )

    def near_copy(a, j, delta):
        src, dst, _ = weights[a]
        return pltpu.make_async_remote_copy(
            src_ref=src.at[j], dst_ref=dst.at[4 - delta],
            send_sem=ws_sem.at[0 if delta == 1 else 1, a], recv_sem=wr_sem.at[0 if delta == 3 else 1, a],
            device_id=peers["y1" if delta == 1 else "y3"], device_id_type=MESH,
        )

    def relay_copy(a, half):
        _, dst, relay = weights[a]
        return pltpu.make_async_remote_copy(
            src_ref=relay, dst_ref=half_of(dst.at[2], half),
            send_sem=relay_send.at[a], recv_sem=wr_sem.at[2 + half, a],
            device_id=peers["y1" if half == 0 else "y3"], device_id_type=MESH,
        )

    def own_copy(a, j):
        src, dst, _ = weights[a]
        return pltpu.make_async_copy(src.at[j], dst.at[0], wl_sem.at[a])

    def pair_copy(a, r):
        _, dst, _ = weights[a]
        return pltpu.make_async_remote_copy(
            src_ref=dst.at[r], dst_ref=dst.at[r],
            send_sem=pair_send.at[r, a], recv_sem=pair_recv.at[r, a],
            device_id=peers["pair"], device_id_type=MESH,
        )

    def each_delta(action, deltas):
        for j in range(2):
            delta_of = lax.rem(2 * core + j + 4 - y, 4)
            for delta in deltas:
                @pl.when(delta_of == delta)
                def _():
                    action(j, delta)

    def start_far(j, delta):
        for a in range(3):
            far_copy(a, j, 0).start()
            far_copy(a, j, 1).start()

    def start_near(j, delta):
        for a in range(3):
            near_copy(a, j, delta).start()

    def start_own(j, delta):
        for a in range(3):
            own_copy(a, j).start()

    def start_weights():
        each_delta(start_far, (2,))
        each_delta(start_near, (1, 3))
        each_delta(start_own, (0,))

    def relay_weights():
        for half in range(2):
            @pl.when(relay_plus if half == 0 else jnp.logical_not(relay_plus))
            def _():
                for a in range(3):
                    far_copy(a, 0, half).wait_recv()
                    relay_copy(a, half).start()

    def pass_near():
        @pl.when(home)
        def _():
            for a in range(3):
                own_copy(a, 0).wait()
                pair_copy(a, 0).start()
            for r in (1, 3):
                for a in range(3):
                    near_copy(a, 0, 4 - r).wait_recv()
                    pair_copy(a, r).start()

    def finish_weights():
        @pl.when(home)
        def _():
            for a in range(3):
                for half in range(2):
                    relay_copy(a, half).wait_recv()
                pair_copy(a, 2).start()
            for r in range(4):
                for a in range(3):
                    pair_copy(a, r).wait_send()

        @pl.when(jnp.logical_not(home))
        def _():
            for r in range(4):
                for a in range(3):
                    pair_copy(a, r).wait_recv()

        def drain_far(j, delta):
            for a in range(3):
                far_copy(a, j, 0).wait_send()
                far_copy(a, j, 1).wait_send()

        def drain_near(j, delta):
            for a in range(3):
                near_copy(a, j, delta).wait_send()

        each_delta(drain_far, (2,))
        each_delta(drain_near, (1, 3))
        for a in range(3):
            relay_copy(a, 0).wait_send()

    def handle(n):
        _, piece, onward = PLAN[n]
        own = piece[1] == 0 and piece[2] == 0
        if own:
            for copy in loads[0:3] if piece[0] == "B" else loads[3:6]:
                copy.wait()
        else:
            arrive(piece)
        for link, target, part in onward:
            copy_on(piece, link, target, part).start()
        hand_over(piece).start()

    owned = [n for n in range(len(PLAN)) if PLAN[n][1][1] == 0 and PLAN[n][1][2] == 0]
    for n in owned:
        handle(n)
    start_weights()

    for m, ref in enumerate((q1_ref, q2_ref)):
        flipped = (ref[...].astype(jnp.float32) * 0.125).T
        row = lax.broadcasted_iota(jnp.int32, flipped.shape, 0)
        for h in range(2):
            mine = (row >= 64 * h) & (row < 64 * (h + 1))
            qt[h, m] = jnp.where(mine, flipped, 0.0).astype(jnp.bfloat16)
    m_ref[...] = jnp.full(m_ref.shape, -1e30, jnp.float32)
    l_ref[...] = jnp.zeros(l_ref.shape, jnp.float32)
    acc_ref[...] = jnp.zeros(acc_ref.shape, jnp.float32)

    def compute(buf, dz):
        rows = buf.shape[1] * buf.shape[2] * buf.shape[3]
        for h in range(2):
            vals = buf[dz, :, :, :, 256 + 128 * h:384 + 128 * h].reshape(rows, 128)
            for m in range(2):
                keys = buf[dz, :, :, :, 128 * m:128 * (m + 1)].reshape(rows, 128)
                scores = jnp.dot(keys, qt[h, m], preferred_element_type=jnp.float32)
                i = h * 2 + m
                old = m_ref[i]
                new = jnp.maximum(old, jnp.max(scores, axis=0, keepdims=True))
                shrink = jnp.exp2((old - new) * log2_e)
                expo = jnp.exp2((scores - new) * log2_e)
                m_ref[i] = new
                l_ref[i] = l_ref[i] * shrink + jnp.sum(expo, axis=0, keepdims=True)
                acc_ref[i] = acc_ref[i] * shrink + lax.dot_general(
                    vals, expo.astype(jnp.bfloat16), (((0,), (0,)), ((), ())),
                    preferred_element_type=jnp.float32,
                )

    def step(t, carry):
        dz = jnp.where(lax.rem(t, 2) == 1, (t + 1) // 2, lax.rem(NZ - (t + 1) // 2, NZ))
        for side, (kind, buf) in enumerate((("B", kvb), ("A", kva))):
            for i in range(NZ):
                u = 2 * i + side

                @pl.when(t == i)
                def _():
                    for n in SLOTS[u]:
                        if n not in owned:
                            handle(n)
                    for piece in PIECES:
                        if (piece[0], piece[1]) == UNITS[u]:
                            hand_over(piece).wait_recv()
                    if u == 7:
                        relay_weights()
                    if u == 13:
                        pass_near()
            compute(buf, dz)
        return carry

    lax.fori_loop(0, NZ, step, 0)

    for h in range(2):
        one = acc_ref[2 * h] / l_ref[2 * h]
        two = acc_ref[2 * h + 1] / l_ref[2 * h + 1]
        joined = one - lam_ref[h] * two
        scale = lax.rsqrt(jnp.mean(joined * joined, axis=0, keepdims=True) + norm_epsilon)
        joined = joined * scale * gain_ref[...]
        att[:, :, 128 * h:128 * (h + 1)] = joined.T.astype(jnp.bfloat16).reshape(4, 64, 128)

    keep = pltpu.make_async_copy(att.at[y], out_ref.at[y], head_recv.at[0])
    keep.start()

    def head_copy(d):
        return pltpu.make_async_remote_copy(
            src_ref=att.at[lax.rem(y + d, 4)], dst_ref=out_ref.at[y],
            send_sem=head_send.at[d], recv_sem=head_recv.at[d],
            device_id=peers[f"y{d}"], device_id_type=MESH,
        )

    for d in (2, 1, 3):
        head_copy(d).start()
    finish_weights()
    for d in (1, 2, 3):
        head_copy(d).wait()
    keep.wait()
    for n, piece in enumerate(PIECES):
        hand_over(piece).wait_send()
        for link, target, part in PLAN[n][2]:
            copy_on(piece, link, target, part).wait_send()


def attend(q1, q2, k1, k2, v, lam, gain, gate, up, down):
    n = len(PIECES)
    bf16 = jnp.bfloat16
    dma = pltpu.SemaphoreType.DMA
    vmem = pl.BlockSpec(memory_space=pltpu.VMEM)
    hbm = pl.BlockSpec(memory_space=pl.ANY)
    _, d, f = gate.shape
    shapes = (
        (4, 64, 256), (4, d, f), (4, d, f), (4, f, d), (d // 2, f), (d // 2, f), (f // 2, d),
    )
    return pl.pallas_call(
        attend_kernel,
        out_shape=[jax.ShapeDtypeStruct(s, bf16) for s in shapes],
        in_specs=[vmem, vmem, hbm, hbm, hbm, pl.BlockSpec(memory_space=pltpu.SMEM), vmem, hbm, hbm, hbm],
        out_specs=[hbm] * 7,
        scratch_shapes=[
            pltpu.VMEM((NZ, 2, 4, ROWS_A, 512), bf16),
            pltpu.VMEM((NZ, 2, 4, ROWS_B, 512), bf16),
            pltpu.VMEM((2, 2, 128, 256), bf16),
            pltpu.VMEM((4, 1, 256), jnp.float32),
            pltpu.VMEM((4, 1, 256), jnp.float32),
            pltpu.VMEM((4, 128, 256), jnp.float32),
            pltpu.VMEM((4, 64, 256), bf16),
            dma((6,)), dma((n,)), dma((n,)), dma((n,)), dma((n,)), dma((4,)), dma((4,)),
            dma((4, 3)), dma((4, 3)), dma((3,)), dma((3,)), dma((3,)), dma((4, 3)), dma((4, 3)),
        ],
        compiler_params=pltpu.CompilerParams(
            collective_id=0, has_side_effects=True, vmem_limit_bytes=60 * 1024 * 1024
        ),
        name="gather_attend",
    )(q1, q2, k1, k2, v, lam, gain, gate, up, down)


def on_device(
    query_one, key_one, query_two, key_two, values, mix_lambda, head_gain, residual_in, out_weight,
    norm_gain, route_ids, route_logits, group_prob, gate_weight, up_weight, down_weight,
):
    heads, wg, wu, wd, _, _, _ = attend(
        query_one, query_two, key_one, key_two, values, mix_lambda, head_gain.reshape(128, 1),
        gate_weight, up_weight, down_weight,
    )
    share, width = residual_in.shape
    top_count = route_ids.shape[1]
    device_count = lax.axis_size("sp") * lax.axis_size("tp")
    token_heads = heads.transpose(1, 0, 2).reshape(share, -1)
    mix = jnp.dot(token_heads, out_weight, preferred_element_type=jnp.float32)
    hidden_f = (residual_in.astype(jnp.float32) + mix).astype(jnp.bfloat16).astype(jnp.float32)
    normed = (
        hidden_f
        * lax.rsqrt(jnp.mean(hidden_f * hidden_f, axis=-1, keepdims=True) + norm_epsilon)
        * norm_gain
    ).astype(jnp.bfloat16)

    flat_ids = route_ids.reshape(-1)
    same = flat_ids[:, None] == flat_ids[None, :]
    count = flat_ids.shape[0]
    before = jnp.arange(count)[None, :] < jnp.arange(count)[:, None]
    rank = jnp.sum((same & before).astype(jnp.int32), axis=1)
    slot_of = ((flat_ids // 4) * 2 + rank) * 4 + flat_ids % 4
    pair_slots = slot_of.reshape(share, top_count)
    places = jnp.arange(device_count, dtype=jnp.int32)
    table = jnp.zeros((device_count, share), jnp.bool_)
    for k in range(top_count):
        table = table | (places[:, None] == pair_slots[None, :, k])
    outgoing = jnp.dot(table.astype(jnp.bfloat16), normed, preferred_element_type=jnp.float32)
    outgoing = outgoing.astype(jnp.bfloat16)
    arrived = lax.all_to_all(outgoing, ("sp", "tp"), 0, 0, tiled=True)
    gate = jnp.einsum("sd,rdf->rsf", arrived, wg, preferred_element_type=jnp.float32)
    upper = jnp.einsum("sd,rdf->rsf", arrived, wu, preferred_element_type=jnp.float32)
    middle = (jax.nn.silu(gate) * upper).astype(jnp.bfloat16)
    parts = jnp.einsum("rsf,rfd->rsd", middle, wd, preferred_element_type=jnp.float32)
    answered = jnp.sum(parts.astype(jnp.bfloat16).astype(jnp.float32), axis=0).astype(jnp.bfloat16)
    returned = lax.all_to_all(answered, ("sp", "tp"), 0, 0, tiled=True)
    picked = returned[slot_of].astype(jnp.float32).reshape(share, top_count, width)
    route_weight = jax.nn.softmax(route_logits, axis=-1) * group_prob[:, None]
    moe = jnp.sum(picked * route_weight[..., None], axis=1)
    return (hidden_f + moe).astype(jnp.bfloat16)


def solution(mesh):
    in_specs = (
        P("sp", "tp"), P("sp", "tp"), P("sp", "tp"), P("sp", "tp"), P("sp", "tp"), P("tp"), P(),
        P(("sp", "tp"), None), P(), P(), P(("sp", "tp"), None), P(("sp", "tp"), None), P(("sp", "tp")),
        P("sp", None, "tp"), P("sp", None, "tp"), P("sp", "tp", None),
    )
    return jax.shard_map(
        on_device, mesh=mesh, in_specs=in_specs, out_specs=P(("sp", "tp"), None), check_vma=False
    )
```

```python
import functools
import math

import jax
import jax.numpy as jnp
from jax import lax
from jax.experimental import pallas as pl
from jax.experimental.pallas import tpu as pltpu
from jax.sharding import PartitionSpec as P

norm_epsilon = 1e-06
MESH = pl.DeviceIdType.MESH
log2_e = math.log2(math.e)

NZ, NX = 8, 4
ROWS_A, ROWS_B = 96, 160
HALF_A, HALF_B = ROWS_A // 2, ROWS_B // 2
UNIT_ORDER = (0, 1, 7, 2, 6, 3, 5, 4)


def gather_plan():
    rate, lag = 46.6, 2.0
    ready, links, sends = {}, {}, []

    def rows_of(piece):
        kind, _, _, part = piece
        whole, half = (ROWS_A, HALF_A) if kind == "A" else (ROWS_B, HALF_B)
        return whole if part < 0 else half

    def follow(piece):
        kind, dz, slot, part = piece
        out = []
        if kind == "A":
            if dz == 0:
                if slot == 0:
                    out += [("x+", ("A", 0, 2, -1), -1), ("x-", ("A", 0, 1, -1), -1)]
                if slot == 2:
                    out.append(("x+", ("A", 0, 3, 0), 0))
                if slot == 1:
                    out.append(("x-", ("A", 0, 3, 1), 1))
                out += [("z+", ("A", 7, slot, part), part), ("z-", ("A", 1, slot, part), part)]
            elif dz in (7, 6) or (dz == 5 and slot < 2):
                out.append(("z+", ("A", dz - 1, slot, part), part))
            elif dz in (1, 2) or (dz == 3 and slot >= 2):
                out.append(("z-", ("A", dz + 1, slot, part), part))
            return out
        if slot == 0:
            if dz == 0:
                out += [("z+", ("B", 7, 0, -1), -1), ("z-", ("B", 1, 0, -1), -1)]
            elif dz in (7, 6):
                out.append(("z+", ("B", dz - 1, 0, -1), -1))
            elif dz in (1, 2):
                out.append(("z-", ("B", dz + 1, 0, -1), -1))
            elif dz == 5:
                out.append(("z+", ("B", 4, 0, 0), 0))
            elif dz == 3:
                out.append(("z-", ("B", 4, 0, 1), 1))
            out += [("x+", ("B", dz, 2, part), part), ("x-", ("B", dz, 1, part), part)]
        elif slot == 2 and dz < 4:
            out.append(("x+", ("B", dz, 3, part), part))
        elif slot == 1 and dz >= 4:
            out.append(("x-", ("B", dz, 3, part), part))
        return out

    events = [(0.0, 1, ("B", 0, 0, -1)), (0.0, 0, ("A", 0, 0, -1))]
    order = []
    while events:
        events.sort()
        now, _, piece = events.pop(0)
        order.append((now, piece, follow(piece)))
        for link, target, _ in follow(piece):
            begin = max(links.get(link, 0.0), now)
            links[link] = begin + rows_of(target) / rate
            events.append((links[link] + lag, len(order), target))
    return order


PLAN = gather_plan()
PIECES = [piece for _, piece, _ in PLAN]
PIECE_INDEX = {piece: n for n, piece in enumerate(PIECES)}
COMPUTE_US = 2.3


def unit_slots():
    units = [(kind, dz) for dz in UNIT_ORDER for kind in ("B", "A")]
    slots, clock, taken = [], 0.0, 0
    for kind, dz in units:
        need = max(t for t, piece, _ in PLAN if piece[0] == kind and piece[1] == dz) + 1.0
        clock = max(clock, need)
        mine = []
        while taken < len(PLAN) and PLAN[taken][0] <= clock:
            mine.append(taken)
            taken += 1
        slots.append(mine)
        clock += COMPUTE_US * (ROWS_A if kind == "A" else ROWS_B) / 128
    assert taken == len(PLAN)
    return units, slots


UNITS, SLOTS = unit_slots()


def attend_kernel(
    q1_ref, q2_ref, k1_ref, k2_ref, v_ref, lam_ref, gain_ref, gate_ref, up_ref, down_ref,
    out_ref, wg_ref, wu_ref, wd_ref, rg_ref, ru_ref, rd_ref,
    kva, kvb, qt, m_ref, l_ref, acc_ref, att, own_gate, own_up, own_down,
    load_sem, send_sem, recv_sem, pass_sem, got_sem, head_send, head_recv,
    ws_sem, wr_sem, wl_sem, relay_sem, relay_send, pair_send, pair_recv,
):
    sp = lax.axis_index("sp")
    y = lax.axis_index("tp")
    core = lax.rem(sp, 2)
    x = lax.rem(sp // 2, NX)
    z = sp // (2 * NX)

    def place(zz, xx, cc):
        return (zz * NX + xx) * 2 + cc

    peers = {
        "x+": (place(z, lax.rem(x + 1, NX), core), y),
        "x-": (place(z, lax.rem(x + NX - 1, NX), core), y),
        "z+": (place(lax.rem(z + 1, NZ), x, core), y),
        "z-": (place(lax.rem(z + NZ - 1, NZ), x, core), y),
        "pair": (place(z, x, 1 - core), y),
        "y1": (sp, lax.rem(y + 1, 4)),
        "y2": (sp, lax.rem(y + 2, 4)),
        "y3": (sp, lax.rem(y + 3, 4)),
    }

    loads = []
    for n, (buf, low, high) in enumerate(((kvb, ROWS_A, 256), (kva, 0, ROWS_A))):
        for c, (ref, lo, hi) in enumerate(((k1_ref, 0, 128), (k2_ref, 128, 256), (v_ref, 256, 512))):
            copy = pltpu.make_async_copy(
                ref.at[low:high], buf.at[0, 0, 0, :, lo:hi], load_sem.at[n * 3 + c]
            )
            copy.start()
            loads.append(copy)

    barrier = pltpu.get_barrier_semaphore()
    for peer in peers.values():
        pl.semaphore_signal(barrier, inc=1, device_id=peer, device_id_type=MESH)
    pl.semaphore_wait(barrier, len(peers))

    def region(piece, side):
        kind, dz, slot, part = piece
        buf, half = (kva, HALF_A) if kind == "A" else (kvb, HALF_B)
        ref = buf.at[dz, side, slot]
        return ref if part < 0 else ref.at[part * half:(part + 1) * half]

    def part_of(piece, part):
        kind, dz, slot, own = piece
        return region(piece, 0) if part == own else region((kind, dz, slot, part), 0)

    def copy_on(piece, link, target, part):
        n = PIECE_INDEX[target]
        return pltpu.make_async_remote_copy(
            src_ref=part_of(piece, part), dst_ref=region(target, 0),
            send_sem=send_sem.at[n], recv_sem=recv_sem.at[n],
            device_id=peers[link], device_id_type=MESH,
        )

    def hand_over(piece):
        n = PIECE_INDEX[piece]
        return pltpu.make_async_remote_copy(
            src_ref=region(piece, 0), dst_ref=region(piece, 1),
            send_sem=pass_sem.at[n], recv_sem=got_sem.at[n],
            device_id=peers["pair"], device_id_type=MESH,
        )

    def arrive(piece):
        n = PIECE_INDEX[piece]
        pltpu.make_async_remote_copy(
            src_ref=region(piece, 0), dst_ref=region(piece, 0),
            send_sem=send_sem.at[n], recv_sem=recv_sem.at[n],
            device_id=peers["pair"], device_id_type=MESH,
        ).wait_recv()

    weights = ((gate_ref, wg_ref, rg_ref), (up_ref, wu_ref, ru_ref), (down_ref, wd_ref, rd_ref))
    home = y // 2 == core
    relay_plus = lax.rem(y + 1, 4) // 2 == core

    def half_of(ref, half):
        rows = ref.shape[0] // 2
        return ref.at[half * rows:(half + 1) * rows]

    def far_copy(a, j, half):
        src, _, relay = weights[a]
        return pltpu.make_async_remote_copy(
            src_ref=half_of(src.at[j], half), dst_ref=relay,
            send_sem=ws_sem.at[2 + half, a], recv_sem=relay_sem.at[a],
            device_id=peers["y1" if half == 0 else "y3"], device_id_type=MESH,
        )

    def near_copy(a, j, delta):
        src, dst, _ = weights[a]
        return pltpu.make_async_remote_copy(
            src_ref=src.at[j], dst_ref=dst.at[4 - delta],
            send_sem=ws_sem.at[0 if delta == 1 else 1, a], recv_sem=wr_sem.at[0 if delta == 3 else 1, a],
            device_id=peers["y1" if delta == 1 else "y3"], device_id_type=MESH,
        )

    def relay_copy(a, half):
        _, dst, relay = weights[a]
        return pltpu.make_async_remote_copy(
            src_ref=relay, dst_ref=half_of(dst.at[2], half),
            send_sem=relay_send.at[a], recv_sem=wr_sem.at[2 + half, a],
            device_id=peers["y1" if half == 0 else "y3"], device_id_type=MESH,
        )

    bounce = (own_gate, own_up, own_down)

    def own_load(a, j):
        return pltpu.make_async_copy(weights[a][0].at[j], bounce[a], wl_sem.at[0, a])

    def own_store(a):
        return pltpu.make_async_copy(bounce[a], weights[a][1].at[0], wl_sem.at[1, a])

    def pair_copy(a, r):
        _, dst, _ = weights[a]
        return pltpu.make_async_remote_copy(
            src_ref=bounce[a] if r == 0 else dst.at[r], dst_ref=dst.at[r],
            send_sem=pair_send.at[r, a], recv_sem=pair_recv.at[r, a],
            device_id=peers["pair"], device_id_type=MESH,
        )

    def each_delta(action, deltas):
        for j in range(2):
            delta_of = lax.rem(2 * core + j + 4 - y, 4)
            for delta in deltas:
                @pl.when(delta_of == delta)
                def _():
                    action(j, delta)

    def start_far(j, delta):
        for a in range(3):
            far_copy(a, j, 0).start()
            far_copy(a, j, 1).start()

    def start_near(j, delta):
        for a in range(3):
            near_copy(a, j, delta).start()

    def start_own(j, delta):
        for a in range(3):
            own_load(a, j).start()

    def start_weights():
        each_delta(start_far, (2,))
        each_delta(start_near, (1, 3))
        each_delta(start_own, (0,))

    def relay_weights():
        for half in range(2):
            @pl.when(relay_plus if half == 0 else jnp.logical_not(relay_plus))
            def _():
                for a in range(3):
                    far_copy(a, 0, half).wait_recv()
                    relay_copy(a, half).start()

    def pass_own():
        @pl.when(home)
        def _():
            for a in range(3):
                own_load(a, 0).wait()
                own_store(a).start()
                pair_copy(a, 0).start()

    def pass_near():
        @pl.when(home)
        def _():
            for r in (1, 3):
                for a in range(3):
                    near_copy(a, 0, 4 - r).wait_recv()
                    pair_copy(a, r).start()

    def finish_weights():
        @pl.when(home)
        def _():
            for a in range(3):
                for half in range(2):
                    relay_copy(a, half).wait_recv()
                pair_copy(a, 2).start()
            for a in range(3):
                own_store(a).wait()
                for r in range(4):
                    pair_copy(a, r).wait_send()

        @pl.when(jnp.logical_not(home))
        def _():
            for r in range(4):
                for a in range(3):
                    pair_copy(a, r).wait_recv()

        def drain_far(j, delta):
            for a in range(3):
                far_copy(a, j, 0).wait_send()
                far_copy(a, j, 1).wait_send()

        def drain_near(j, delta):
            for a in range(3):
                near_copy(a, j, delta).wait_send()

        each_delta(drain_far, (2,))
        each_delta(drain_near, (1, 3))
        for a in range(3):
            relay_copy(a, 0).wait_send()

    def handle(n):
        _, piece, onward = PLAN[n]
        own = piece[1] == 0 and piece[2] == 0
        if own:
            for copy in loads[0:3] if piece[0] == "B" else loads[3:6]:
                copy.wait()
        else:
            arrive(piece)
        for link, target, part in onward:
            copy_on(piece, link, target, part).start()
        hand_over(piece).start()

    owned = [n for n in range(len(PLAN)) if PLAN[n][1][1] == 0 and PLAN[n][1][2] == 0]
    for n in owned:
        handle(n)
    start_weights()

    for m, ref in enumerate((q1_ref, q2_ref)):
        flipped = (ref[...].astype(jnp.float32) * 0.125).T
        row = lax.broadcasted_iota(jnp.int32, flipped.shape, 0)
        for h in range(2):
            mine = (row >= 64 * h) & (row < 64 * (h + 1))
            qt[h, m] = jnp.where(mine, flipped, 0.0).astype(jnp.bfloat16)
    m_ref[...] = jnp.full(m_ref.shape, -1e30, jnp.float32)
    l_ref[...] = jnp.zeros(l_ref.shape, jnp.float32)
    acc_ref[...] = jnp.zeros(acc_ref.shape, jnp.float32)

    def compute(buf, dz):
        rows = buf.shape[1] * buf.shape[2] * buf.shape[3]
        for h in range(2):
            vals = buf[dz, :, :, :, 256 + 128 * h:384 + 128 * h].reshape(rows, 128)
            for m in range(2):
                keys = buf[dz, :, :, :, 128 * m:128 * (m + 1)].reshape(rows, 128)
                scores = jnp.dot(keys, qt[h, m], preferred_element_type=jnp.float32)
                i = h * 2 + m
                old = m_ref[i]
                new = jnp.maximum(old, jnp.max(scores, axis=0, keepdims=True))
                shrink = jnp.exp2((old - new) * log2_e)
                expo = jnp.exp2((scores - new) * log2_e)
                m_ref[i] = new
                l_ref[i] = l_ref[i] * shrink + jnp.sum(expo, axis=0, keepdims=True)
                acc_ref[i] = acc_ref[i] * shrink + lax.dot_general(
                    vals, expo.astype(jnp.bfloat16), (((0,), (0,)), ((), ())),
                    preferred_element_type=jnp.float32,
                )

    def step(t, carry):
        dz = jnp.where(lax.rem(t, 2) == 1, (t + 1) // 2, lax.rem(NZ - (t + 1) // 2, NZ))
        for side, (kind, buf) in enumerate((("B", kvb), ("A", kva))):
            for i in range(NZ):
                u = 2 * i + side

                @pl.when(t == i)
                def _():
                    for n in SLOTS[u]:
                        if n not in owned:
                            handle(n)
                    for piece in PIECES:
                        if (piece[0], piece[1]) == UNITS[u]:
                            hand_over(piece).wait_recv()
                    if u == 0:
                        pass_own()
                    if u == 7:
                        relay_weights()
                    if u == 13:
                        pass_near()
            compute(buf, dz)
        return carry

    lax.fori_loop(0, NZ, step, 0)

    for h in range(2):
        one = acc_ref[2 * h] / l_ref[2 * h]
        two = acc_ref[2 * h + 1] / l_ref[2 * h + 1]
        joined = one - lam_ref[h] * two
        scale = lax.rsqrt(jnp.mean(joined * joined, axis=0, keepdims=True) + norm_epsilon)
        joined = joined * scale * gain_ref[...]
        att[:, :, 128 * h:128 * (h + 1)] = joined.T.astype(jnp.bfloat16).reshape(4, 64, 128)

    keep = pltpu.make_async_copy(att.at[y], out_ref.at[y], head_recv.at[0])
    keep.start()

    def head_copy(d):
        return pltpu.make_async_remote_copy(
            src_ref=att.at[lax.rem(y + d, 4)], dst_ref=out_ref.at[y],
            send_sem=head_send.at[d], recv_sem=head_recv.at[d],
            device_id=peers[f"y{d}"], device_id_type=MESH,
        )

    for d in (2, 1, 3):
        head_copy(d).start()
    finish_weights()
    for d in (1, 2, 3):
        head_copy(d).wait()
    keep.wait()
    for n, piece in enumerate(PIECES):
        hand_over(piece).wait_send()
        for link, target, part in PLAN[n][2]:
            copy_on(piece, link, target, part).wait_send()


def attend(q1, q2, k1, k2, v, lam, gain, gate, up, down):
    n = len(PIECES)
    bf16 = jnp.bfloat16
    dma = pltpu.SemaphoreType.DMA
    vmem = pl.BlockSpec(memory_space=pltpu.VMEM)
    hbm = pl.BlockSpec(memory_space=pl.ANY)
    _, d, f = gate.shape
    shapes = (
        (4, 64, 256), (4, d, f), (4, d, f), (4, f, d), (d // 2, f), (d // 2, f), (f // 2, d),
    )
    return pl.pallas_call(
        attend_kernel,
        out_shape=[jax.ShapeDtypeStruct(s, bf16) for s in shapes],
        in_specs=[vmem, vmem, hbm, hbm, hbm, pl.BlockSpec(memory_space=pltpu.SMEM), vmem, hbm, hbm, hbm],
        out_specs=[hbm] * 7,
        scratch_shapes=[
            pltpu.VMEM((NZ, 2, 4, ROWS_A, 512), bf16),
            pltpu.VMEM((NZ, 2, 4, ROWS_B, 512), bf16),
            pltpu.VMEM((2, 2, 128, 256), bf16),
            pltpu.VMEM((4, 1, 256), jnp.float32),
            pltpu.VMEM((4, 1, 256), jnp.float32),
            pltpu.VMEM((4, 128, 256), jnp.float32),
            pltpu.VMEM((4, 64, 256), bf16),
            pltpu.VMEM((d, f), bf16), pltpu.VMEM((d, f), bf16), pltpu.VMEM((f, d), bf16),
            dma((6,)), dma((n,)), dma((n,)), dma((n,)), dma((n,)), dma((4,)), dma((4,)),
            dma((4, 3)), dma((4, 3)), dma((2, 3)), dma((3,)), dma((3,)), dma((4, 3)), dma((4, 3)),
        ],
        compiler_params=pltpu.CompilerParams(
            collective_id=0, has_side_effects=True, vmem_limit_bytes=60 * 1024 * 1024
        ),
        name="gather_attend",
    )(q1, q2, k1, k2, v, lam, gain, gate, up, down)


def expert_kernel(
    heads_ref, resid_ref, proj_ref, norm_ref, pair_ref, slot_ref, weight_ref, wg_ref, wu_ref, wd_ref,
    out_ref,
    proj, vg, vu, vd, spread, outgoing, arrived, rows, total, answer, returned, hidden,
    load_sem, go_sem, come_sem, back_sem, return_sem,
):
    sp = lax.axis_index("sp")
    y = lax.axis_index("tp")
    core = lax.rem(sp, 2)
    x = lax.rem(sp // 2, NX)
    z = sp // (2 * NX)
    here = sp * 4 + y
    devices = outgoing.shape[0]
    group = devices // 2

    loads = [pltpu.make_async_copy(proj_ref, proj, load_sem.at[3])]
    for n, (src, dst) in enumerate(((wg_ref, vg), (wu_ref, vu), (wd_ref, vd))):
        loads.append(pltpu.make_async_copy(src, dst, load_sem.at[n]))
    for load in loads:
        load.start()

    def offset(i, sign):
        dz, dy, dx, dc = lax.rem(i, NZ), lax.rem(i // NZ, 4), lax.rem(i // (4 * NZ), NX), i // group
        zz = lax.rem(z + sign * dz + NZ, NZ)
        xx = lax.rem(x + sign * dx + NX, NX)
        yy = lax.rem(y + sign * dy + 4, 4)
        cc = lax.rem(core + dc, 2)
        return (zz * NX + xx) * 2 + cc, yy

    barrier = pltpu.get_barrier_semaphore()

    def greet(i, carry):
        pl.semaphore_signal(barrier, inc=1, device_id=offset(i, 1), device_id_type=MESH)
        return carry

    lax.fori_loop(1, devices, greet, 0)

    loads[0].wait()
    mix = jnp.dot(heads_ref[0], proj[0], preferred_element_type=jnp.float32)
    for t in range(1, 4):
        mix = mix + jnp.dot(heads_ref[t], proj[t], preferred_element_type=jnp.float32)
    kept = (resid_ref[...].astype(jnp.float32) + mix).astype(jnp.bfloat16).astype(jnp.float32)
    scale = lax.rsqrt(jnp.mean(kept * kept, axis=-1, keepdims=True) + norm_epsilon)
    normed = (kept * scale * norm_ref[...]).astype(jnp.bfloat16)
    place = lax.broadcasted_iota(jnp.int32, (devices, kept.shape[0]), 0)
    table = ((place == pair_ref[0:1, :]) | (place == pair_ref[1:2, :])).astype(jnp.bfloat16)
    for k in range(16):
        cols = slice(128 * k, 128 * (k + 1))
        hidden[:, k, :] = kept[:, cols]
        spread[:, k, :] = jnp.dot(table, normed[:, cols], preferred_element_type=jnp.float32)
    outgoing[...] = spread[...].astype(jnp.bfloat16)
    arrived[0] = outgoing[here]

    pl.semaphore_wait(barrier, devices - 1)

    def send(i, carry):
        sp_to, y_to = offset(i, 1)
        pltpu.make_async_remote_copy(
            src_ref=outgoing.at[sp_to * 4 + y_to], dst_ref=arrived.at[i],
            send_sem=go_sem.at[0], recv_sem=come_sem.at[i // group],
            device_id=(sp_to, y_to), device_id_type=MESH,
        ).start()
        return carry

    lax.fori_loop(1, devices, send, 0)

    def whole(ref, low, high, send_sem, recv_sem):
        return pltpu.make_async_remote_copy(
            src_ref=ref.at[low:high], dst_ref=ref.at[low:high], send_sem=send_sem, recv_sem=recv_sem,
            device_id=(sp, lax.rem(y + 1, 4)), device_id_type=MESH,
        )

    for load in loads[1:]:
        load.wait()

    def work(g, carry):
        for n in range(2):
            @pl.when(g == n)
            def _():
                whole(arrived, 1 - n, group, go_sem.at[0], come_sem.at[n]).wait_recv()
        block = pl.ds(pl.multiple_of(g * group, group), group)
        spread[0:group] = arrived[block].astype(jnp.float32)
        for k in range(16):
            rows[:, 128 * k:128 * (k + 1)] = spread[0:group, k, :].astype(jnp.bfloat16)
        for r in range(4):
            gate = jnp.dot(rows[...], vg[r], preferred_element_type=jnp.float32)
            upper = jnp.dot(rows[...], vu[r], preferred_element_type=jnp.float32)
            middle = (gate / (1.0 + jnp.exp(-gate)) * upper).astype(jnp.bfloat16)
            part = jnp.dot(middle, vd[r], preferred_element_type=jnp.float32)
            part = part.astype(jnp.bfloat16).astype(jnp.float32)
            if r == 0:
                total[...] = part
            else:
                total[...] = total[...] + part
        for k in range(16):
            spread[0:group, k, :] = total[:, 128 * k:128 * (k + 1)]
        answer[block] = spread[0:group].astype(jnp.bfloat16)

        def reply(i, inner):
            sp_to, y_to = offset(i, -1)
            pltpu.make_async_remote_copy(
                src_ref=answer.at[i], dst_ref=returned.at[here],
                send_sem=back_sem.at[0], recv_sem=return_sem.at[0],
                device_id=(sp_to, y_to), device_id_type=MESH,
            ).start()
            return inner

        lax.fori_loop(jnp.maximum(g * group, 1), (g + 1) * group, reply, 0)
        return carry

    lax.fori_loop(0, 2, work, 0)
    returned[here] = answer[0]
    whole(returned, 0, devices - 1, back_sem.at[0], return_sem.at[0]).wait_recv()

    def combine(t, carry):
        joined = hidden[t]
        for k in range(2):
            joined = joined + returned[slot_ref[2 * t + k]].astype(jnp.float32) * weight_ref[2 * t + k]
        out_ref[t] = joined.astype(jnp.bfloat16)
        return carry

    lax.fori_loop(0, out_ref.shape[0], combine, 0)
    whole(outgoing, 0, devices - 1, go_sem.at[0], come_sem.at[0]).wait_send()
    whole(answer, 0, devices - 1, back_sem.at[0], return_sem.at[0]).wait_send()


def run_experts(heads, resid, proj, norm, pair_slots, slots, route_weight, wg, wu, wd):
    bf16, f32 = jnp.bfloat16, jnp.float32
    dma = pltpu.SemaphoreType.DMA
    vmem = pl.BlockSpec(memory_space=pltpu.VMEM)
    smem = pl.BlockSpec(memory_space=pltpu.SMEM)
    hbm = pl.BlockSpec(memory_space=pl.ANY)
    share, width = resid.shape
    devices = lax.axis_size("sp") * lax.axis_size("tp")
    tiles = (width // 128, 128)
    return pl.pallas_call(
        expert_kernel,
        out_shape=jax.ShapeDtypeStruct((share,) + tiles, bf16),
        in_specs=[vmem, vmem, hbm, vmem, vmem, smem, smem, hbm, hbm, hbm],
        out_specs=vmem,
        scratch_shapes=[
            pltpu.VMEM(proj.shape, bf16),
            pltpu.VMEM(wg.shape, bf16), pltpu.VMEM(wu.shape, bf16), pltpu.VMEM(wd.shape, bf16),
            pltpu.VMEM((devices,) + tiles, f32),
            pltpu.VMEM((devices,) + tiles, bf16),
            pltpu.VMEM((devices,) + tiles, bf16),
            pltpu.VMEM((devices // 2, width), bf16),
            pltpu.VMEM((devices // 2, width), f32),
            pltpu.VMEM((devices,) + tiles, bf16),
            pltpu.VMEM((devices,) + tiles, bf16),
            pltpu.VMEM((share,) + tiles, f32),
            dma((4,)), dma((1,)), dma((2,)), dma((1,)), dma((1,)),
        ],
        compiler_params=pltpu.CompilerParams(
            collective_id=1, has_side_effects=True, vmem_limit_bytes=48 * 1024 * 1024
        ),
        name="experts",
    )(heads, resid, proj, norm, pair_slots, slots, route_weight, wg, wu, wd)


def on_device(
    query_one, key_one, query_two, key_two, values, mix_lambda, head_gain, residual_in, out_weight,
    norm_gain, route_ids, route_logits, group_prob, gate_weight, up_weight, down_weight,
):
    heads, wg, wu, wd, _, _, _ = attend(
        query_one, query_two, key_one, key_two, values, mix_lambda, head_gain.reshape(128, 1),
        gate_weight, up_weight, down_weight,
    )
    share, width = residual_in.shape
    flat_ids = route_ids.reshape(-1)
    count = flat_ids.shape[0]
    same = flat_ids[:, None] == flat_ids[None, :]
    before = jnp.arange(count)[None, :] < jnp.arange(count)[:, None]
    rank = jnp.sum((same & before).astype(jnp.int32), axis=1)
    slots = ((flat_ids // 4) * 2 + rank) * 4 + flat_ids % 4
    route_weight = jax.nn.softmax(route_logits, axis=-1) * group_prob[:, None]
    out = run_experts(
        heads, residual_in, out_weight.reshape(4, -1, width), norm_gain.reshape(1, width),
        slots.reshape(share, -1).T, slots, route_weight.reshape(-1), wg, wu, wd,
    )
    return out.reshape(share, width)


def solution(mesh):
    in_specs = (
        P("sp", "tp"), P("sp", "tp"), P("sp", "tp"), P("sp", "tp"), P("sp", "tp"), P("tp"), P(),
        P(("sp", "tp"), None), P(), P(), P(("sp", "tp"), None), P(("sp", "tp"), None), P(("sp", "tp")),
        P("sp", None, "tp"), P("sp", None, "tp"), P("sp", "tp", None),
    )
    return jax.shard_map(
        on_device, mesh=mesh, in_specs=in_specs, out_specs=P(("sp", "tp"), None), check_vma=False
    )
```

```python
import functools
import math

import jax
import jax.numpy as jnp
from jax import lax
from jax.experimental import pallas as pl
from jax.experimental.pallas import tpu as pltpu
from jax.sharding import PartitionSpec as P

norm_epsilon = 1e-06
MESH = pl.DeviceIdType.MESH
log2_e = math.log2(math.e)

NZ, NX = 8, 4
ROWS_A, ROWS_B = 96, 160
HALF_A, HALF_B = ROWS_A // 2, ROWS_B // 2


def gather_plan():
    def rows_of(piece):
        kind, _, _, part = piece
        whole, half = (ROWS_A, HALF_A) if kind == "A" else (ROWS_B, HALF_B)
        return whole if part < 0 else half

    def follow(piece):
        kind, dz, slot, part = piece
        out = []
        if kind == "A":
            if dz == 0:
                if slot == 0:
                    out += [("x+", ("A", 0, 2, -1), -1), ("x-", ("A", 0, 1, -1), -1)]
                if slot == 2:
                    out.append(("x+", ("A", 0, 3, 0), 0))
                if slot == 1:
                    out.append(("x-", ("A", 0, 3, 1), 1))
                out += [("z+", ("A", 7, slot, part), part), ("z-", ("A", 1, slot, part), part)]
            elif dz in (7, 6) or (dz == 5 and slot < 2):
                out.append(("z+", ("A", dz - 1, slot, part), part))
            elif dz in (1, 2) or (dz == 3 and slot >= 2):
                out.append(("z-", ("A", dz + 1, slot, part), part))
            return out
        if slot == 0:
            if dz == 0:
                out += [("z+", ("B", 7, 0, -1), -1), ("z-", ("B", 1, 0, -1), -1)]
            elif dz in (7, 6):
                out.append(("z+", ("B", dz - 1, 0, -1), -1))
            elif dz in (1, 2):
                out.append(("z-", ("B", dz + 1, 0, -1), -1))
            elif dz == 5:
                out.append(("z+", ("B", 4, 0, 0), 0))
            elif dz == 3:
                out.append(("z-", ("B", 4, 0, 1), 1))
            out += [("x+", ("B", dz, 2, part), part), ("x-", ("B", dz, 1, part), part)]
        elif slot == 2 and dz < 4:
            out.append(("x+", ("B", dz, 3, part), part))
        elif slot == 1 and dz >= 4:
            out.append(("x-", ("B", dz, 3, part), part))
        return out

    rate, lag, pair_rate, pair_lag, half_step, issue = 46.6, 3.0, 500.0, 1.5, 1.25, 0.05
    links, coming = {}, [(0.0, 0, ("B", 0, 0, -1)), (0.0, 1, ("A", 0, 0, -1))]
    plan, blocks, slots, now, serial = [], {"A": [], "B": []}, [[]], 2.0, 2
    missing, shared = {}, {}
    for kind in "AB":
        for dz in range(NZ):
            for slot in range(4):
                missing[kind, dz, slot] = 2 if halved((kind, dz, slot)) else 1
    while len(slots) <= 2 * STEPS:
        coming.sort()
        if coming and coming[0][0] <= now:
            _, _, piece = coming.pop(0)
            slots[-1].append(len(plan))
            onward = follow(piece)
            plan.append((piece, onward))
            now += issue
            for link, target, _ in onward:
                links[link] = max(links.get(link, 0.0), now) + rows_of(target) / rate
                serial += 1
                coming.append((links[link] + lag, serial, target))
            links["pair"] = max(links.get("pair", 0.0), now) + rows_of(piece) / pair_rate
            block = piece[:3]
            missing[block] -= 1
            shared[block] = links["pair"] + pair_lag
            if missing[block] == 0:
                blocks[piece[0]].append(block)
            continue
        done = (len(slots) - 1) // 2
        need = [blocks[kind][k] for kind in "AB" for k in (2 * done, 2 * done + 1) if k < len(blocks[kind])]
        begin = max(shared[block] for block in need) if len(need) == 4 else None
        if begin is not None and begin <= now:
            now += half_step
            slots.append([])
        else:
            now = min([t for t in (begin, coming[0][0] if coming else None) if t is not None])
    return plan, blocks, slots, now


def halved(block):
    kind, dz, slot = block
    if kind == "A":
        return slot == 3
    return dz == 4


STEPS = 16
PLAN, BLOCKS, SLOTS, PLANNED_US = gather_plan()
PIECES = [piece for piece, _ in PLAN]
PIECE_INDEX = {piece: n for n, piece in enumerate(PIECES)}


def attend_kernel(
    q1_ref, q2_ref, k1_ref, k2_ref, v_ref, lam_ref, gain_ref, gate_ref, up_ref, down_ref,
    out_ref, wg_ref, wu_ref, wd_ref,
    kva, kvb, qt, m_ref, l_ref, acc_ref, att, own_gate, own_up, own_down,
    load_sem, send_sem, recv_sem, pass_sem, got_sem, head_send, head_recv,
    ws_sem, wr_sem, wl_sem, pair_send, pair_recv,
):
    sp = lax.axis_index("sp")
    y = lax.axis_index("tp")
    core = lax.rem(sp, 2)
    x = lax.rem(sp // 2, NX)
    z = sp // (2 * NX)

    def place(zz, xx, cc):
        return (zz * NX + xx) * 2 + cc

    peers = {
        "x+": (place(z, lax.rem(x + 1, NX), core), y),
        "x-": (place(z, lax.rem(x + NX - 1, NX), core), y),
        "z+": (place(lax.rem(z + 1, NZ), x, core), y),
        "z-": (place(lax.rem(z + NZ - 1, NZ), x, core), y),
        "pair": (place(z, x, 1 - core), y),
        "y1": (sp, lax.rem(y + 1, 4)),
        "y2": (sp, lax.rem(y + 2, 4)),
        "y3": (sp, lax.rem(y + 3, 4)),
    }

    loads = []
    for n, (buf, low, high) in enumerate(((kvb, ROWS_A, 256), (kva, 0, ROWS_A))):
        for c, (ref, lo, hi) in enumerate(((k1_ref, 0, 128), (k2_ref, 128, 256), (v_ref, 256, 512))):
            copy = pltpu.make_async_copy(
                ref.at[low:high], buf.at[0, 0, :, lo:hi], load_sem.at[n * 3 + c]
            )
            copy.start()
            loads.append(copy)

    barrier = pltpu.get_barrier_semaphore()
    for peer in peers.values():
        pl.semaphore_signal(barrier, inc=1, device_id=peer, device_id_type=MESH)
    pl.semaphore_wait(barrier, len(peers))

    def region(piece, side):
        kind, dz, slot, part = piece
        buf, half = (kva, HALF_A) if kind == "A" else (kvb, HALF_B)
        ref = buf.at[4 * dz + slot, side]
        return ref if part < 0 else ref.at[part * half:(part + 1) * half]

    def part_of(piece, part):
        kind, dz, slot, own = piece
        return region(piece, 0) if part == own else region((kind, dz, slot, part), 0)

    def copy_on(piece, link, target, part):
        n = PIECE_INDEX[target]
        return pltpu.make_async_remote_copy(
            src_ref=part_of(piece, part), dst_ref=region(target, 0),
            send_sem=send_sem.at[n], recv_sem=recv_sem.at[n],
            device_id=peers[link], device_id_type=MESH,
        )

    def hand_over(piece):
        n = PIECE_INDEX[piece]
        return pltpu.make_async_remote_copy(
            src_ref=region(piece, 0), dst_ref=region(piece, 1),
            send_sem=pass_sem.at[n], recv_sem=got_sem.at[n],
            device_id=peers["pair"], device_id_type=MESH,
        )

    def arrive(piece):
        n = PIECE_INDEX[piece]
        pltpu.make_async_remote_copy(
            src_ref=region(piece, 0), dst_ref=region(piece, 0),
            send_sem=send_sem.at[n], recv_sem=recv_sem.at[n],
            device_id=peers["pair"], device_id_type=MESH,
        ).wait_recv()

    weights = ((gate_ref, wg_ref), (up_ref, wu_ref), (down_ref, wd_ref))
    bounce = (own_gate, own_up, own_down)
    home = y // 2 == core

    def slice_copy(a, j, delta):
        src, dst = weights[a]
        return pltpu.make_async_remote_copy(
            src_ref=src.at[j], dst_ref=dst.at[4 - delta],
            send_sem=ws_sem.at[delta - 1, a], recv_sem=wr_sem.at[3 - delta, a],
            device_id=peers[f"y{delta}"], device_id_type=MESH,
        )

    def own_load(a, j):
        return pltpu.make_async_copy(weights[a][0].at[j], bounce[a], wl_sem.at[0, a])

    def own_store(a):
        return pltpu.make_async_copy(bounce[a], weights[a][1].at[0], wl_sem.at[1, a])

    def pair_copy(a, r):
        _, dst = weights[a]
        return pltpu.make_async_remote_copy(
            src_ref=bounce[a] if r == 0 else dst.at[r], dst_ref=dst.at[r],
            send_sem=pair_send.at[r, a], recv_sem=pair_recv.at[r, a],
            device_id=peers["pair"], device_id_type=MESH,
        )

    def each_delta(action, deltas):
        for j in range(2):
            delta_of = lax.rem(2 * core + j + 4 - y, 4)
            for delta in deltas:
                @pl.when(delta_of == delta)
                def _():
                    action(j, delta)

    def start_weights():
        for a in range(3):
            each_delta(lambda j, delta: slice_copy(a, j, delta).start(), (1, 2, 3))
            each_delta(lambda j, delta: own_load(a, j).start(), (0,))

    def pass_own():
        @pl.when(home)
        def _():
            for a in range(3):
                own_load(a, 0).wait()
                own_store(a).start()
                pair_copy(a, 0).start()

    def pass_slices(a):
        @pl.when(home)
        def _():
            for r in (1, 3, 2):
                slice_copy(a, 0, 4 - r).wait_recv()
                pair_copy(a, r).start()

    def finish_weights():
        @pl.when(home)
        def _():
            for a in range(3):
                own_store(a).wait()
                for r in range(4):
                    pair_copy(a, r).wait_send()

        @pl.when(jnp.logical_not(home))
        def _():
            for r in range(4):
                for a in range(3):
                    pair_copy(a, r).wait_recv()

        for a in range(3):
            each_delta(lambda j, delta: slice_copy(a, j, delta).wait_send(), (1, 2, 3))

    def handle(n):
        piece, onward = PLAN[n]
        own = piece[1] == 0 and piece[2] == 0
        if own:
            for copy in loads[0:3] if piece[0] == "B" else loads[3:6]:
                copy.wait()
        else:
            arrive(piece)
        for link, target, part in onward:
            copy_on(piece, link, target, part).start()
        hand_over(piece).start()

    owned = [n for n in range(len(PLAN)) if PIECES[n][1] == 0 and PIECES[n][2] == 0]
    for n in owned:
        handle(n)
    start_weights()

    for m, ref in enumerate((q1_ref, q2_ref)):
        flipped = (ref[...].astype(jnp.float32) * 0.125).T
        row = lax.broadcasted_iota(jnp.int32, flipped.shape, 0)
        for h in range(2):
            mine = (row >= 64 * h) & (row < 64 * (h + 1))
            qt[h, m] = jnp.where(mine, flipped, 0.0).astype(jnp.bfloat16)
    m_ref[...] = jnp.full(m_ref.shape, -1e30, jnp.float32)
    l_ref[...] = jnp.zeros(l_ref.shape, jnp.float32)
    acc_ref[...] = jnp.zeros(acc_ref.shape, jnp.float32)

    def compute(picked, h):
        def columns(low):
            return jnp.concatenate([
                buf[b, :, :, low:low + 128].reshape(-1, 128) for buf, b in picked
            ], axis=0)

        vals = columns(256 + 128 * h)
        for m in range(2):
            scores = jnp.dot(columns(128 * m), qt[h, m], preferred_element_type=jnp.float32)
            i = h * 2 + m
            old = m_ref[i]
            new = jnp.maximum(old, jnp.max(scores, axis=0, keepdims=True))
            shrink = jnp.exp2((old - new) * log2_e)
            expo = jnp.exp2((scores - new) * log2_e)
            m_ref[i] = new
            l_ref[i] = l_ref[i] * shrink + jnp.sum(expo, axis=0, keepdims=True)
            acc_ref[i] = acc_ref[i] * shrink + lax.dot_general(
                vals, expo.astype(jnp.bfloat16), (((0,), (0,)), ((), ())),
                preferred_element_type=jnp.float32,
            )

    def chosen(t, kind, k):
        index = jnp.int32(0)
        for i in range(STEPS):
            _, dz, slot = BLOCKS[kind][2 * i + k]
            index = jnp.where(t == i, 4 * dz + slot, index)
        return index

    def step(t, carry):
        picked = [(buf, chosen(t, kind, k)) for kind, buf in (("A", kva), ("B", kvb)) for k in range(2)]
        for h in range(2):
            for i in range(STEPS):
                @pl.when(t == i)
                def _():
                    for n in SLOTS[2 * i + h]:
                        if n not in owned:
                            handle(n)
                    if h == 0:
                        for piece in PIECES:
                            if piece[:3] in BLOCKS[piece[0]][2 * i:2 * i + 2]:
                                hand_over(piece).wait_recv()
                    if (i, h) == (0, 0):
                        pass_own()
                    if (i, h) == (8, 1):
                        pass_slices(0)
                    if (i, h) == (13, 1):
                        pass_slices(1)
            compute(picked, h)
        return carry

    lax.fori_loop(0, STEPS, step, 0)

    for h in range(2):
        one = acc_ref[2 * h] / l_ref[2 * h]
        two = acc_ref[2 * h + 1] / l_ref[2 * h + 1]
        joined = one - lam_ref[h] * two
        scale = lax.rsqrt(jnp.mean(joined * joined, axis=0, keepdims=True) + norm_epsilon)
        joined = (joined * scale).T * gain_ref[...]
        att[:, :, 128 * h:128 * (h + 1)] = joined.astype(jnp.bfloat16).reshape(4, 64, 128)

    keep = pltpu.make_async_copy(att.at[y], out_ref.at[y], head_recv.at[0])
    keep.start()

    def head_copy(d):
        return pltpu.make_async_remote_copy(
            src_ref=att.at[lax.rem(y + d, 4)], dst_ref=out_ref.at[y],
            send_sem=head_send.at[d], recv_sem=head_recv.at[d],
            device_id=peers[f"y{d}"], device_id_type=MESH,
        )

    for d in (2, 1, 3):
        head_copy(d).start()
    pass_slices(2)
    finish_weights()
    for d in (1, 2, 3):
        head_copy(d).wait()
    keep.wait()
    for n, piece in enumerate(PIECES):
        hand_over(piece).wait_send()
        for link, target, part in PLAN[n][1]:
            copy_on(piece, link, target, part).wait_send()


def attend(q1, q2, k1, k2, v, lam, gain, gate, up, down):
    n = len(PIECES)
    bf16 = jnp.bfloat16
    dma = pltpu.SemaphoreType.DMA
    vmem = pl.BlockSpec(memory_space=pltpu.VMEM)
    hbm = pl.BlockSpec(memory_space=pl.ANY)
    _, d, f = gate.shape
    shapes = ((4, 64, 256), (4, d, f), (4, d, f), (4, f, d))
    return pl.pallas_call(
        attend_kernel,
        out_shape=[jax.ShapeDtypeStruct(s, bf16) for s in shapes],
        in_specs=[vmem, vmem, hbm, hbm, hbm, pl.BlockSpec(memory_space=pltpu.SMEM), vmem, hbm, hbm, hbm],
        out_specs=[hbm] * 4,
        scratch_shapes=[
            pltpu.VMEM((NZ * 4, 2, ROWS_A, 512), bf16),
            pltpu.VMEM((NZ * 4, 2, ROWS_B, 512), bf16),
            pltpu.VMEM((2, 2, 128, 256), bf16),
            pltpu.VMEM((4, 1, 256), jnp.float32),
            pltpu.VMEM((4, 1, 256), jnp.float32),
            pltpu.VMEM((4, 128, 256), jnp.float32),
            pltpu.VMEM((4, 64, 256), bf16),
            pltpu.VMEM((d, f), bf16), pltpu.VMEM((d, f), bf16), pltpu.VMEM((f, d), bf16),
            dma((6,)), dma((n,)), dma((n,)), dma((n,)), dma((n,)), dma((4,)), dma((4,)),
            dma((3, 3)), dma((3, 3)), dma((2, 3)), dma((4, 3)), dma((4, 3)),
        ],
        compiler_params=pltpu.CompilerParams(
            collective_id=0, has_side_effects=True, vmem_limit_bytes=60 * 1024 * 1024,
        ),
        name="gather_attend",
    )(q1, q2, k1, k2, v, lam, gain, gate, up, down)


def expert_kernel(
    heads_ref, resid_ref, proj_ref, norm_ref, pair_ref, slot_ref, weight_ref, wg_ref, wu_ref, wd_ref,
    out_ref,
    proj, vg, vu, vd, spread, outgoing, arrived, rows, total, answer, returned, hidden,
    load_sem, go_sem, come_sem, back_sem, return_sem,
):
    sp = lax.axis_index("sp")
    y = lax.axis_index("tp")
    core = lax.rem(sp, 2)
    x = lax.rem(sp // 2, NX)
    z = sp // (2 * NX)
    here = sp * 4 + y
    devices = outgoing.shape[0]
    group = devices // 2

    loads = [pltpu.make_async_copy(proj_ref, proj, load_sem.at[3])]
    for n, (src, dst) in enumerate(((wg_ref, vg), (wu_ref, vu), (wd_ref, vd))):
        loads.append(pltpu.make_async_copy(src, dst, load_sem.at[n]))
    loads[0].start()
    ahead = [lax.rem(z + dz, NZ) * NX * 2 for dz in range(NZ)]
    behind = [ahead[(NZ - dz) % NZ] for dz in range(NZ)]

    def each_peer(low, high, sign, action):
        bases = ahead if sign > 0 else behind

        def some(q, carry):
            dy, dx, dc = lax.rem(q, 4), lax.rem(q // 4, NX), q // (4 * NX)
            xx = lax.rem(x + sign * dx + NX, NX)
            yy = lax.rem(y + sign * dy + 4, 4)
            offset = xx * 2 + lax.rem(core + dc, 2)
            for dz in range(NZ):
                if dz == 0:
                    @pl.when(q > 0)
                    def _():
                        action(q * NZ, bases[0] + offset, yy)
                else:
                    action(q * NZ + dz, bases[dz] + offset, yy)
            return carry

        lax.fori_loop(low, high, some, 0)

    barrier = pltpu.get_barrier_semaphore()

    def greet(i, sp_to, y_to):
        pl.semaphore_signal(barrier, inc=1, device_id=(sp_to, y_to), device_id_type=MESH)

    each_peer(0, devices // NZ, 1, greet)
    loads[0].wait()
    for load in loads[1:]:
        load.start()
    mix = jnp.dot(heads_ref[0], proj[0], preferred_element_type=jnp.float32)
    for t in range(1, 4):
        mix = mix + jnp.dot(heads_ref[t], proj[t], preferred_element_type=jnp.float32)
    kept = (resid_ref[...].astype(jnp.float32) + mix).astype(jnp.bfloat16).astype(jnp.float32)
    scale = lax.rsqrt(jnp.mean(kept * kept, axis=-1, keepdims=True) + norm_epsilon)
    normed = (kept * scale * norm_ref[...]).astype(jnp.bfloat16)
    place = lax.broadcasted_iota(jnp.int32, (devices, kept.shape[0]), 0)
    table = ((place == pair_ref[0:1, :]) | (place == pair_ref[1:2, :])).astype(jnp.bfloat16)
    for k in range(16):
        cols = slice(128 * k, 128 * (k + 1))
        hidden[:, k, :] = kept[:, cols]
        spread[:, k, :] = jnp.dot(table, normed[:, cols], preferred_element_type=jnp.float32)
    outgoing[...] = spread[...].astype(jnp.bfloat16)
    arrived[0] = outgoing[here]

    pl.semaphore_wait(barrier, devices - 1)

    def send(i, sp_to, y_to, n):
        pltpu.make_async_remote_copy(
            src_ref=outgoing.at[sp_to * 4 + y_to], dst_ref=arrived.at[i],
            send_sem=go_sem.at[0], recv_sem=come_sem.at[n],
            device_id=(sp_to, y_to), device_id_type=MESH,
        ).start()

    for n in range(2):
        each_peer(n * group // NZ, (n + 1) * group // NZ, 1, functools.partial(send, n=n))

    def whole(ref, low, high, send_sem, recv_sem):
        return pltpu.make_async_remote_copy(
            src_ref=ref.at[low:high], dst_ref=ref.at[low:high], send_sem=send_sem, recv_sem=recv_sem,
            device_id=(sp, lax.rem(y + 1, 4)), device_id_type=MESH,
        )

    for load in loads[1:]:
        load.wait()

    def work(g, carry):
        for n in range(2):
            @pl.when(g == n)
            def _():
                whole(arrived, 1 - n, group, go_sem.at[0], come_sem.at[n]).wait_recv()
        block = pl.ds(pl.multiple_of(g * group, group), group)
        spread[0:group] = arrived[block].astype(jnp.float32)
        for k in range(16):
            rows[:, 128 * k:128 * (k + 1)] = spread[0:group, k, :].astype(jnp.bfloat16)
        for r in range(4):
            gate = jnp.dot(rows[...], vg[r], preferred_element_type=jnp.float32)
            upper = jnp.dot(rows[...], vu[r], preferred_element_type=jnp.float32)
            middle = (gate / (1.0 + jnp.exp(-gate)) * upper).astype(jnp.bfloat16)
            part = jnp.dot(middle, vd[r], preferred_element_type=jnp.float32)
            part = part.astype(jnp.bfloat16).astype(jnp.float32)
            if r == 0:
                total[...] = part
            else:
                total[...] = total[...] + part
        for k in range(16):
            spread[0:group, k, :] = total[:, 128 * k:128 * (k + 1)]
        answer[block] = spread[0:group].astype(jnp.bfloat16)

        def reply(i, sp_to, y_to):
            pltpu.make_async_remote_copy(
                src_ref=answer.at[i], dst_ref=returned.at[here],
                send_sem=back_sem.at[0], recv_sem=return_sem.at[0],
                device_id=(sp_to, y_to), device_id_type=MESH,
            ).start()

        each_peer(g * (group // NZ), (g + 1) * (group // NZ), -1, reply)
        return carry

    lax.fori_loop(0, 2, work, 0)
    returned[here] = answer[0]
    whole(returned, 0, devices - 1, back_sem.at[0], return_sem.at[0]).wait_recv()

    def combine(t, carry):
        joined = hidden[t]
        for k in range(2):
            joined = joined + returned[slot_ref[2 * t + k]].astype(jnp.float32) * weight_ref[2 * t + k]
        out_ref[t] = joined.astype(jnp.bfloat16)
        return carry

    lax.fori_loop(0, out_ref.shape[0], combine, 0)
    whole(outgoing, 0, devices - 1, go_sem.at[0], come_sem.at[0]).wait_send()
    whole(answer, 0, devices - 1, back_sem.at[0], return_sem.at[0]).wait_send()


def run_experts(heads, resid, proj, norm, pair_slots, slots, route_weight, wg, wu, wd):
    bf16, f32 = jnp.bfloat16, jnp.float32
    dma = pltpu.SemaphoreType.DMA
    vmem = pl.BlockSpec(memory_space=pltpu.VMEM)
    smem = pl.BlockSpec(memory_space=pltpu.SMEM)
    hbm = pl.BlockSpec(memory_space=pl.ANY)
    share, width = resid.shape
    devices = lax.axis_size("sp") * lax.axis_size("tp")
    tiles = (width // 128, 128)
    return pl.pallas_call(
        expert_kernel,
        out_shape=jax.ShapeDtypeStruct((share,) + tiles, bf16),
        in_specs=[vmem, vmem, hbm, vmem, vmem, smem, smem, hbm, hbm, hbm],
        out_specs=vmem,
        scratch_shapes=[
            pltpu.VMEM(proj.shape, bf16),
            pltpu.VMEM(wg.shape, bf16), pltpu.VMEM(wu.shape, bf16), pltpu.VMEM(wd.shape, bf16),
            pltpu.VMEM((devices,) + tiles, f32),
            pltpu.VMEM((devices,) + tiles, bf16),
            pltpu.VMEM((devices,) + tiles, bf16),
            pltpu.VMEM((devices // 2, width), bf16),
            pltpu.VMEM((devices // 2, width), f32),
            pltpu.VMEM((devices,) + tiles, bf16),
            pltpu.VMEM((devices,) + tiles, bf16),
            pltpu.VMEM((share,) + tiles, f32),
            dma((4,)), dma((1,)), dma((2,)), dma((1,)), dma((1,)),
        ],
        compiler_params=pltpu.CompilerParams(
            collective_id=1, has_side_effects=True, vmem_limit_bytes=60 * 1024 * 1024
        ),
        name="experts",
    )(heads, resid, proj, norm, pair_slots, slots, route_weight, wg, wu, wd)


def on_device(
    query_one, key_one, query_two, key_two, values, mix_lambda, head_gain, residual_in, out_weight,
    norm_gain, route_ids, route_logits, group_prob, gate_weight, up_weight, down_weight,
):
    heads, wg, wu, wd = attend(
        query_one, query_two, key_one, key_two, values, mix_lambda, head_gain.reshape(1, 128),
        gate_weight, up_weight, down_weight,
    )
    share, width = residual_in.shape
    heads, route_ids, route_logits, group_prob = lax.optimization_barrier(
        (heads, route_ids, route_logits, group_prob)
    )
    flat_ids = route_ids.reshape(-1)
    count = flat_ids.shape[0]
    same = flat_ids[:, None] == flat_ids[None, :]
    before = jnp.arange(count)[None, :] < jnp.arange(count)[:, None]
    rank = jnp.sum((same & before).astype(jnp.int32), axis=1)
    slots = ((flat_ids // 4) * 2 + rank) * 4 + flat_ids % 4
    route_weight = jax.nn.softmax(route_logits, axis=-1) * group_prob[:, None]
    out = run_experts(
        heads, residual_in, out_weight.reshape(4, -1, width), norm_gain.reshape(1, width),
        slots.reshape(share, -1).T, slots, route_weight.reshape(-1), wg, wu, wd,
    )
    return out.reshape(share, width)


def solution(mesh):
    in_specs = (
        P("sp", "tp"), P("sp", "tp"), P("sp", "tp"), P("sp", "tp"), P("sp", "tp"), P("tp"), P(),
        P(("sp", "tp"), None), P(), P(), P(("sp", "tp"), None), P(("sp", "tp"), None), P(("sp", "tp")),
        P("sp", None, "tp"), P("sp", None, "tp"), P("sp", "tp", None),
    )
    return jax.shard_map(
        on_device, mesh=mesh, in_specs=in_specs, out_specs=P(("sp", "tp"), None), check_vma=False
    )
```

```python
import functools
import math

import jax
import jax.numpy as jnp
from jax import lax
from jax.experimental import pallas as pl
from jax.experimental.pallas import tpu as pltpu
from jax.sharding import PartitionSpec as P

norm_epsilon = 1e-06
MESH = pl.DeviceIdType.MESH
log2_e = math.log2(math.e)

NZ, NX = 8, 4
ROWS_A, ROWS_B = 96, 160
HALF_A, HALF_B = ROWS_A // 2, ROWS_B // 2


def gather_plan():
    def rows_of(piece):
        kind, _, _, part = piece
        whole, half = (ROWS_A, HALF_A) if kind == "A" else (ROWS_B, HALF_B)
        return whole if part < 0 else half

    def follow(piece):
        kind, dz, slot, part = piece
        out = []
        if kind == "A":
            if dz == 0:
                if slot == 0:
                    out += [("x+", ("A", 0, 2, -1), -1), ("x-", ("A", 0, 1, -1), -1)]
                if slot == 2:
                    out.append(("x+", ("A", 0, 3, 0), 0))
                if slot == 1:
                    out.append(("x-", ("A", 0, 3, 1), 1))
                out += [("z+", ("A", 7, slot, part), part), ("z-", ("A", 1, slot, part), part)]
            elif dz in (7, 6) or (dz == 5 and slot < 2):
                out.append(("z+", ("A", dz - 1, slot, part), part))
            elif dz in (1, 2) or (dz == 3 and slot >= 2):
                out.append(("z-", ("A", dz + 1, slot, part), part))
            return out
        if slot == 0:
            if dz == 0:
                out += [("z+", ("B", 7, 0, -1), -1), ("z-", ("B", 1, 0, -1), -1)]
            elif dz in (7, 6):
                out.append(("z+", ("B", dz - 1, 0, -1), -1))
            elif dz in (1, 2):
                out.append(("z-", ("B", dz + 1, 0, -1), -1))
            elif dz == 5:
                out.append(("z+", ("B", 4, 0, 0), 0))
            elif dz == 3:
                out.append(("z-", ("B", 4, 0, 1), 1))
            out += [("x+", ("B", dz, 2, part), part), ("x-", ("B", dz, 1, part), part)]
        elif slot == 2 and dz < 4:
            out.append(("x+", ("B", dz, 3, part), part))
        elif slot == 1 and dz >= 4:
            out.append(("x-", ("B", dz, 3, part), part))
        return out

    rate, lag, pair_rate, pair_lag, half_step, issue = 46.6, 3.0, 500.0, 1.5, 1.25, 0.05
    links, coming = {}, [(0.0, 0, ("B", 0, 0, -1)), (0.0, 1, ("A", 0, 0, -1))]
    plan, blocks, slots, now, serial = [], {"A": [], "B": []}, [[]], 2.0, 2
    missing, shared = {}, {}
    for kind in "AB":
        for dz in range(NZ):
            for slot in range(4):
                missing[kind, dz, slot] = 2 if halved((kind, dz, slot)) else 1
    while len(slots) <= 2 * STEPS:
        coming.sort()
        if coming and coming[0][0] <= now:
            _, _, piece = coming.pop(0)
            slots[-1].append(len(plan))
            onward = follow(piece)
            plan.append((piece, onward))
            now += issue
            for link, target, _ in onward:
                links[link] = max(links.get(link, 0.0), now) + rows_of(target) / rate
                serial += 1
                coming.append((links[link] + lag, serial, target))
            links["pair"] = max(links.get("pair", 0.0), now) + rows_of(piece) / pair_rate
            block = piece[:3]
            missing[block] -= 1
            shared[block] = links["pair"] + pair_lag
            if missing[block] == 0:
                blocks[piece[0]].append(block)
            continue
        done = (len(slots) - 1) // 2
        need = [blocks[kind][k] for kind in "AB" for k in (2 * done, 2 * done + 1) if k < len(blocks[kind])]
        begin = max(shared[block] for block in need) if len(need) == 4 else None
        if begin is not None and begin <= now:
            now += half_step
            slots.append([])
        else:
            now = min([t for t in (begin, coming[0][0] if coming else None) if t is not None])
    return plan, blocks, slots, now


def halved(block):
    kind, dz, slot = block
    if kind == "A":
        return slot == 3
    return dz == 4


STEPS = 16
PLAN, BLOCKS, SLOTS, PLANNED_US = gather_plan()
PIECES = [piece for piece, _ in PLAN]
PIECE_INDEX = {piece: n for n, piece in enumerate(PIECES)}


def attend_kernel(
    q1_ref, q2_ref, k1_ref, k2_ref, v_ref, lam_ref, gain_ref, gate_ref, up_ref, down_ref,
    out_ref, wg_ref, wu_ref, wd_ref,
    kva, kvb, qt, m_ref, l_ref, acc_ref, att, own_gate, own_up, own_down,
    load_sem, send_sem, recv_sem, pass_sem, got_sem, head_send, head_recv,
    ws_sem, wr_sem, wl_sem, pair_send, pair_recv,
):
    sp = lax.axis_index("sp")
    y = lax.axis_index("tp")
    core = lax.rem(sp, 2)
    x = lax.rem(sp // 2, NX)
    z = sp // (2 * NX)

    def place(zz, xx, cc):
        return (zz * NX + xx) * 2 + cc

    peers = {
        "x+": (place(z, lax.rem(x + 1, NX), core), y),
        "x-": (place(z, lax.rem(x + NX - 1, NX), core), y),
        "z+": (place(lax.rem(z + 1, NZ), x, core), y),
        "z-": (place(lax.rem(z + NZ - 1, NZ), x, core), y),
        "pair": (place(z, x, 1 - core), y),
        "y1": (sp, lax.rem(y + 1, 4)),
        "y2": (sp, lax.rem(y + 2, 4)),
        "y3": (sp, lax.rem(y + 3, 4)),
    }

    loads = []
    for n, (buf, low, high) in enumerate(((kvb, ROWS_A, 256), (kva, 0, ROWS_A))):
        for c, (ref, lo, hi) in enumerate(((k1_ref, 0, 128), (k2_ref, 128, 256), (v_ref, 256, 512))):
            copy = pltpu.make_async_copy(
                ref.at[low:high], buf.at[0, 0, :, lo:hi], load_sem.at[n * 3 + c]
            )
            copy.start()
            loads.append(copy)

    barrier = pltpu.get_barrier_semaphore()
    for peer in peers.values():
        pl.semaphore_signal(barrier, inc=1, device_id=peer, device_id_type=MESH)
    pl.semaphore_wait(barrier, len(peers))

    def region(piece, side):
        kind, dz, slot, part = piece
        buf, half = (kva, HALF_A) if kind == "A" else (kvb, HALF_B)
        ref = buf.at[4 * dz + slot, side]
        return ref if part < 0 else ref.at[part * half:(part + 1) * half]

    def part_of(piece, part):
        kind, dz, slot, own = piece
        return region(piece, 0) if part == own else region((kind, dz, slot, part), 0)

    def copy_on(piece, link, target, part):
        n = PIECE_INDEX[target]
        return pltpu.make_async_remote_copy(
            src_ref=part_of(piece, part), dst_ref=region(target, 0),
            send_sem=send_sem.at[n], recv_sem=recv_sem.at[n],
            device_id=peers[link], device_id_type=MESH,
        )

    def hand_over(piece):
        n = PIECE_INDEX[piece]
        return pltpu.make_async_remote_copy(
            src_ref=region(piece, 0), dst_ref=region(piece, 1),
            send_sem=pass_sem.at[n], recv_sem=got_sem.at[n],
            device_id=peers["pair"], device_id_type=MESH,
        )

    def arrive(piece):
        n = PIECE_INDEX[piece]
        pltpu.make_async_remote_copy(
            src_ref=region(piece, 0), dst_ref=region(piece, 0),
            send_sem=send_sem.at[n], recv_sem=recv_sem.at[n],
            device_id=peers["pair"], device_id_type=MESH,
        ).wait_recv()

    weights = ((gate_ref, wg_ref), (up_ref, wu_ref), (down_ref, wd_ref))
    bounce = (own_gate, own_up, own_down)
    pieces = 2 * len(weights)

    def half_of(ref, a):
        rows = ref.shape[0] // 2
        return ref.at[(a % 2) * rows:(a % 2 + 1) * rows]

    def source(a, j):
        return half_of(weights[a // 2][0].at[j], a)

    def target(a, r):
        return half_of(weights[a // 2][1].at[r], a)

    def bounced(a):
        return half_of(bounce[a // 2], a)
    home = y // 2 == core

    def slice_copy(a, j, delta):
        return pltpu.make_async_remote_copy(
            src_ref=source(a, j), dst_ref=target(a, 4 - delta),
            send_sem=ws_sem.at[delta - 1, a], recv_sem=wr_sem.at[3 - delta, a],
            device_id=peers[f"y{delta}"], device_id_type=MESH,
        )

    def own_load(a, j):
        return pltpu.make_async_copy(source(a, j), bounced(a), wl_sem.at[0, a])

    def own_store(a):
        return pltpu.make_async_copy(bounced(a), target(a, 0), wl_sem.at[1, a])

    def pair_copy(a, r):
        return pltpu.make_async_remote_copy(
            src_ref=bounced(a) if r == 0 else target(a, r), dst_ref=target(a, r),
            send_sem=pair_send.at[r, a], recv_sem=pair_recv.at[r, a],
            device_id=peers["pair"], device_id_type=MESH,
        )

    def each_delta(action, deltas):
        for j in range(2):
            delta_of = lax.rem(2 * core + j + 4 - y, 4)
            for delta in deltas:
                @pl.when(delta_of == delta)
                def _():
                    action(j, delta)

    def start_weights():
        for a in range(pieces):
            each_delta(lambda j, delta: slice_copy(a, j, delta).start(), (1, 2, 3))
            each_delta(lambda j, delta: own_load(a, j).start(), (0,))

    def pass_own():
        @pl.when(home)
        def _():
            for a in range(pieces):
                own_load(a, 0).wait()
                own_store(a).start()
                pair_copy(a, 0).start()

    def pass_slices(a):
        @pl.when(home)
        def _():
            for r in (1, 3, 2):
                slice_copy(a, 0, 4 - r).wait_recv()
                pair_copy(a, r).start()

    def finish_weights():
        @pl.when(home)
        def _():
            for a in range(pieces):
                own_store(a).wait()
                for r in range(4):
                    pair_copy(a, r).wait_send()

        @pl.when(jnp.logical_not(home))
        def _():
            for r in range(4):
                for a in range(pieces):
                    pair_copy(a, r).wait_recv()

        for a in range(pieces):
            each_delta(lambda j, delta: slice_copy(a, j, delta).wait_send(), (1, 2, 3))

    def handle(n):
        piece, onward = PLAN[n]
        own = piece[1] == 0 and piece[2] == 0
        if own:
            for copy in loads[0:3] if piece[0] == "B" else loads[3:6]:
                copy.wait()
        else:
            arrive(piece)
        for link, target, part in onward:
            copy_on(piece, link, target, part).start()
        hand_over(piece).start()

    owned = [n for n in range(len(PLAN)) if PIECES[n][1] == 0 and PIECES[n][2] == 0]
    for n in owned:
        handle(n)
    start_weights()

    for m, ref in enumerate((q1_ref, q2_ref)):
        flipped = (ref[...].astype(jnp.float32) * 0.125).T
        row = lax.broadcasted_iota(jnp.int32, flipped.shape, 0)
        for h in range(2):
            mine = (row >= 64 * h) & (row < 64 * (h + 1))
            qt[h, m] = jnp.where(mine, flipped, 0.0).astype(jnp.bfloat16)
    m_ref[...] = jnp.full(m_ref.shape, -1e30, jnp.float32)
    l_ref[...] = jnp.zeros(l_ref.shape, jnp.float32)
    acc_ref[...] = jnp.zeros(acc_ref.shape, jnp.float32)

    def compute(picked, h):
        def columns(low):
            return jnp.concatenate([
                buf[b, :, :, low:low + 128].reshape(-1, 128) for buf, b in picked
            ], axis=0)

        vals = columns(256 + 128 * h)
        for m in range(2):
            scores = jnp.dot(columns(128 * m), qt[h, m], preferred_element_type=jnp.float32)
            i = h * 2 + m
            old = m_ref[i]
            new = jnp.maximum(old, jnp.max(scores, axis=0, keepdims=True))
            shrink = jnp.exp2((old - new) * log2_e)
            expo = jnp.exp2((scores - new) * log2_e)
            m_ref[i] = new
            l_ref[i] = l_ref[i] * shrink + jnp.sum(expo, axis=0, keepdims=True)
            acc_ref[i] = acc_ref[i] * shrink + lax.dot_general(
                vals, expo.astype(jnp.bfloat16), (((0,), (0,)), ((), ())),
                preferred_element_type=jnp.float32,
            )

    def chosen(t, kind, k):
        index = jnp.int32(0)
        for i in range(STEPS):
            _, dz, slot = BLOCKS[kind][2 * i + k]
            index = jnp.where(t == i, 4 * dz + slot, index)
        return index

    def step(t, carry):
        picked = [(buf, chosen(t, kind, k)) for kind, buf in (("A", kva), ("B", kvb)) for k in range(2)]
        for h in range(2):
            for i in range(STEPS):
                @pl.when(t == i)
                def _():
                    for n in SLOTS[2 * i + h]:
                        if n not in owned:
                            handle(n)
                    if h == 0:
                        for piece in PIECES:
                            if piece[:3] in BLOCKS[piece[0]][2 * i:2 * i + 2]:
                                hand_over(piece).wait_recv()
                    if (i, h) == (0, 0):
                        pass_own()
                    if (i, h) == (8, 1):
                        pass_slices(0)
                        pass_slices(1)
                    if (i, h) == (13, 1):
                        pass_slices(2)
                        pass_slices(3)
            compute(picked, h)
        return carry

    lax.fori_loop(0, STEPS, step, 0)

    for h in range(2):
        one = acc_ref[2 * h] / l_ref[2 * h]
        two = acc_ref[2 * h + 1] / l_ref[2 * h + 1]
        joined = one - lam_ref[h] * two
        scale = lax.rsqrt(jnp.mean(joined * joined, axis=0, keepdims=True) + norm_epsilon)
        joined = (joined * scale).T * gain_ref[...]
        att[:, :, 128 * h:128 * (h + 1)] = joined.astype(jnp.bfloat16).reshape(4, 64, 128)

    keep = pltpu.make_async_copy(att.at[y], out_ref.at[y], head_recv.at[0])
    keep.start()

    def head_copy(d):
        return pltpu.make_async_remote_copy(
            src_ref=att.at[lax.rem(y + d, 4)], dst_ref=out_ref.at[y],
            send_sem=head_send.at[d], recv_sem=head_recv.at[d],
            device_id=peers[f"y{d}"], device_id_type=MESH,
        )

    for d in (2, 1, 3):
        head_copy(d).start()
    pass_slices(4)
    pass_slices(5)
    finish_weights()
    for d in (1, 2, 3):
        head_copy(d).wait()
    keep.wait()
    for n, piece in enumerate(PIECES):
        hand_over(piece).wait_send()
        for link, target, part in PLAN[n][1]:
            copy_on(piece, link, target, part).wait_send()


def attend(q1, q2, k1, k2, v, lam, gain, gate, up, down):
    n = len(PIECES)
    bf16 = jnp.bfloat16
    dma = pltpu.SemaphoreType.DMA
    vmem = pl.BlockSpec(memory_space=pltpu.VMEM)
    hbm = pl.BlockSpec(memory_space=pl.ANY)
    _, d, f = gate.shape
    shapes = ((4, 64, 256), (4, d, f), (4, d, f), (4, f, d))
    return pl.pallas_call(
        attend_kernel,
        out_shape=[jax.ShapeDtypeStruct(s, bf16) for s in shapes],
        in_specs=[vmem, vmem, hbm, hbm, hbm, pl.BlockSpec(memory_space=pltpu.SMEM), vmem, hbm, hbm, hbm],
        out_specs=[hbm] * 4,
        scratch_shapes=[
            pltpu.VMEM((NZ * 4, 2, ROWS_A, 512), bf16),
            pltpu.VMEM((NZ * 4, 2, ROWS_B, 512), bf16),
            pltpu.VMEM((2, 2, 128, 256), bf16),
            pltpu.VMEM((4, 1, 256), jnp.float32),
            pltpu.VMEM((4, 1, 256), jnp.float32),
            pltpu.VMEM((4, 128, 256), jnp.float32),
            pltpu.VMEM((4, 64, 256), bf16),
            pltpu.VMEM((d, f), bf16), pltpu.VMEM((d, f), bf16), pltpu.VMEM((f, d), bf16),
            dma((6,)), dma((n,)), dma((n,)), dma((n,)), dma((n,)), dma((4,)), dma((4,)),
            dma((3, 6)), dma((3, 6)), dma((2, 6)), dma((4, 6)), dma((4, 6)),
        ],
        compiler_params=pltpu.CompilerParams(
            collective_id=0, has_side_effects=True, vmem_limit_bytes=60 * 1024 * 1024,
        ),
        name="gather_attend",
    )(q1, q2, k1, k2, v, lam, gain, gate, up, down)


def expert_kernel(
    heads_ref, resid_ref, proj_ref, norm_ref, pair_ref, slot_ref, weight_ref, wg_ref, wu_ref, wd_ref,
    out_ref,
    proj, vg, vu, vd, spread, outgoing, arrived, rows, total, answer, returned, hidden,
    load_sem, go_sem, come_sem, back_sem, return_sem,
):
    sp = lax.axis_index("sp")
    y = lax.axis_index("tp")
    core = lax.rem(sp, 2)
    x = lax.rem(sp // 2, NX)
    z = sp // (2 * NX)
    here = sp * 4 + y
    devices, share = outgoing.shape[0], out_ref.shape[0]
    group = devices // 2

    loads = [pltpu.make_async_copy(proj_ref, proj, load_sem.at[3])]
    for n, (src, dst) in enumerate(((wg_ref, vg), (wu_ref, vu), (wd_ref, vd))):
        loads.append(pltpu.make_async_copy(src, dst, load_sem.at[n]))
    loads[0].start()
    ahead = [lax.rem(z + dz, NZ) * NX * 2 for dz in range(NZ)]
    behind = [ahead[(NZ - dz) % NZ] for dz in range(NZ)]

    def each_peer(low, high, sign, action):
        bases = ahead if sign > 0 else behind

        def some(q, carry):
            dy, dx, dc = lax.rem(q, 4), lax.rem(q // 4, NX), q // (4 * NX)
            xx = lax.rem(x + sign * dx + NX, NX)
            yy = lax.rem(y + sign * dy + 4, 4)
            offset = xx * 2 + lax.rem(core + dc, 2)
            for dz in range(NZ):
                if dz == 0:
                    @pl.when(q > 0)
                    def _():
                        action(q * NZ, bases[0] + offset, yy)
                else:
                    action(q * NZ + dz, bases[dz] + offset, yy)
            return carry

        lax.fori_loop(low, high, some, 0)

    barrier = pltpu.get_barrier_semaphore()

    def greet(i, sp_to, y_to):
        pl.semaphore_signal(barrier, inc=1, device_id=(sp_to, y_to), device_id_type=MESH)

    each_peer(0, devices // NZ, 1, greet)
    loads[0].wait()
    for load in loads[1:]:
        load.start()
    mix = jnp.dot(heads_ref[0], proj[0], preferred_element_type=jnp.float32)
    for t in range(1, 4):
        mix = mix + jnp.dot(heads_ref[t], proj[t], preferred_element_type=jnp.float32)
    kept = (resid_ref[...].astype(jnp.float32) + mix).astype(jnp.bfloat16).astype(jnp.float32)
    scale = lax.rsqrt(jnp.mean(kept * kept, axis=-1, keepdims=True) + norm_epsilon)
    normed = (kept * scale * norm_ref[...]).astype(jnp.bfloat16)
    place = lax.broadcasted_iota(jnp.int32, (devices, pair_ref.shape[1]), 0)
    table = (place == pair_ref[...]).astype(jnp.bfloat16)
    normed = jnp.concatenate([normed, normed], axis=0)
    for k in range(16):
        cols = slice(128 * k, 128 * (k + 1))
        hidden[:, k, :] = kept[:, cols]
        spread[:, k, :] = jnp.dot(table, normed[:, cols], preferred_element_type=jnp.float32)
    outgoing[...] = spread[...].astype(jnp.bfloat16)
    arrived[0] = outgoing[here]

    pl.semaphore_wait(barrier, devices - 1)

    def send(i, sp_to, y_to, n):
        pltpu.make_async_remote_copy(
            src_ref=outgoing.at[sp_to * 4 + y_to], dst_ref=arrived.at[i],
            send_sem=go_sem.at[0], recv_sem=come_sem.at[n],
            device_id=(sp_to, y_to), device_id_type=MESH,
        ).start()

    for n in range(2):
        each_peer(n * group // NZ, (n + 1) * group // NZ, 1, functools.partial(send, n=n))

    def whole(ref, low, high, send_sem, recv_sem):
        return pltpu.make_async_remote_copy(
            src_ref=ref.at[low:high], dst_ref=ref.at[low:high], send_sem=send_sem, recv_sem=recv_sem,
            device_id=(sp, lax.rem(y + 1, 4)), device_id_type=MESH,
        )

    for load in loads[1:]:
        load.wait()

    def work(g, carry):
        for n in range(2):
            @pl.when(g == n)
            def _():
                whole(arrived, 1 - n, group, go_sem.at[0], come_sem.at[n]).wait_recv()
        block = pl.ds(pl.multiple_of(g * group, group), group)
        spread[0:group] = arrived[block].astype(jnp.float32)
        for k in range(16):
            rows[:, 128 * k:128 * (k + 1)] = spread[0:group, k, :].astype(jnp.bfloat16)
        for r in range(4):
            gate = jnp.dot(rows[...], vg[r], preferred_element_type=jnp.float32)
            upper = jnp.dot(rows[...], vu[r], preferred_element_type=jnp.float32)
            middle = (gate / (1.0 + jnp.exp(-gate)) * upper).astype(jnp.bfloat16)
            part = jnp.dot(middle, vd[r], preferred_element_type=jnp.float32)
            part = part.astype(jnp.bfloat16).astype(jnp.float32)
            if r == 0:
                total[...] = part
            else:
                total[...] = total[...] + part
        for k in range(16):
            spread[0:group, k, :] = total[:, 128 * k:128 * (k + 1)]
        answer[block] = spread[0:group].astype(jnp.bfloat16)

        def reply(i, sp_to, y_to):
            pltpu.make_async_remote_copy(
                src_ref=answer.at[i], dst_ref=returned.at[here],
                send_sem=back_sem.at[0], recv_sem=return_sem.at[0],
                device_id=(sp_to, y_to), device_id_type=MESH,
            ).start()

        each_peer(g * (group // NZ), (g + 1) * (group // NZ), -1, reply)
        return carry

    lax.fori_loop(0, 2, work, 0)
    returned[here] = answer[0]
    whole(returned, 0, devices - 1, back_sem.at[0], return_sem.at[0]).wait_recv()

    def combine(t, carry):
        joined = hidden[t]
        for k in range(2):
            joined = joined + returned[slot_ref[k * share + t]].astype(jnp.float32) * weight_ref[k * share + t]
        out_ref[t] = joined.astype(jnp.bfloat16)
        return carry

    lax.fori_loop(0, out_ref.shape[0], combine, 0)
    whole(outgoing, 0, devices - 1, go_sem.at[0], come_sem.at[0]).wait_send()
    whole(answer, 0, devices - 1, back_sem.at[0], return_sem.at[0]).wait_send()


def run_experts(heads, resid, proj, norm, pair_slots, slots, route_weight, wg, wu, wd):
    bf16, f32 = jnp.bfloat16, jnp.float32
    dma = pltpu.SemaphoreType.DMA
    vmem = pl.BlockSpec(memory_space=pltpu.VMEM)
    smem = pl.BlockSpec(memory_space=pltpu.SMEM)
    hbm = pl.BlockSpec(memory_space=pl.ANY)
    share, width = resid.shape
    devices = lax.axis_size("sp") * lax.axis_size("tp")
    tiles = (width // 128, 128)
    return pl.pallas_call(
        expert_kernel,
        out_shape=jax.ShapeDtypeStruct((share,) + tiles, bf16),
        in_specs=[vmem, vmem, hbm, vmem, vmem, smem, smem, hbm, hbm, hbm],
        out_specs=vmem,
        scratch_shapes=[
            pltpu.VMEM(proj.shape, bf16),
            pltpu.VMEM(wg.shape, bf16), pltpu.VMEM(wu.shape, bf16), pltpu.VMEM(wd.shape, bf16),
            pltpu.VMEM((devices,) + tiles, f32),
            pltpu.VMEM((devices,) + tiles, bf16),
            pltpu.VMEM((devices,) + tiles, bf16),
            pltpu.VMEM((devices // 2, width), bf16),
            pltpu.VMEM((devices // 2, width), f32),
            pltpu.VMEM((devices,) + tiles, bf16),
            pltpu.VMEM((devices,) + tiles, bf16),
            pltpu.VMEM((share,) + tiles, f32),
            dma((4,)), dma((1,)), dma((2,)), dma((1,)), dma((1,)),
        ],
        compiler_params=pltpu.CompilerParams(
            collective_id=1, has_side_effects=True, vmem_limit_bytes=60 * 1024 * 1024,
        ),
        name="experts",
    )(heads, resid, proj, norm, pair_slots, slots, route_weight, wg, wu, wd)


def on_device(
    query_one, key_one, query_two, key_two, values, mix_lambda, head_gain, residual_in, out_weight,
    norm_gain, route_ids, route_logits, group_prob, gate_weight, up_weight, down_weight,
):
    heads, wg, wu, wd = attend(
        query_one, query_two, key_one, key_two, values, mix_lambda, head_gain.reshape(1, 128),
        gate_weight, up_weight, down_weight,
    )
    share, width = residual_in.shape
    heads, route_ids, route_logits, group_prob = lax.optimization_barrier(
        (heads, route_ids, route_logits, group_prob)
    )
    flat_ids = route_ids.T.reshape(-1)
    count = flat_ids.shape[0]
    same = flat_ids[:, None] == flat_ids[None, :]
    before = jnp.arange(count)[None, :] < jnp.arange(count)[:, None]
    rank = jnp.sum((same & before).astype(jnp.int32), axis=1)
    slots = ((flat_ids // 4) * 2 + rank) * 4 + flat_ids % 4
    route_weight = jax.nn.softmax(route_logits.T, axis=0) * group_prob[None, :]
    out = run_experts(
        heads, residual_in, out_weight.reshape(4, -1, width), norm_gain.reshape(1, width),
        slots.reshape(1, -1), slots, route_weight.reshape(-1), wg, wu, wd,
    )
    return out.reshape(share, width)


def solution(mesh):
    in_specs = (
        P("sp", "tp"), P("sp", "tp"), P("sp", "tp"), P("sp", "tp"), P("sp", "tp"), P("tp"), P(),
        P(("sp", "tp"), None), P(), P(), P(("sp", "tp"), None), P(("sp", "tp"), None), P(("sp", "tp")),
        P("sp", None, "tp"), P("sp", None, "tp"), P("sp", "tp", None),
    )
    return jax.shard_map(
        on_device, mesh=mesh, in_specs=in_specs, out_specs=P(("sp", "tp"), None), check_vma=False
    )
```
